32 devices in a mesh: fs: 4 (over z), rep: 4 (over y, x), tp: 2 (over core).
Axes of the slice: x: 2, y: 2, z: 4, core: 2. Of those that a mesh axis runs over, the one named last changes fastest.
Arguments:
- input_act: bfloat16 [12288, 2048], P(('fs', 'rep')), may hold values from -6 to 6
- query_cot: bfloat16 [12288, 1024], P(('fs', 'rep'), 'tp'), may hold values from -6 to 6
- out_cot: bfloat16 [12288, 2048], P(('fs', 'rep')), may hold values from -6 to 6
- attn_out: bfloat16 [12288, 1024], P(('fs', 'rep'), 'tp'), may hold values from -6 to 6
- query_w: float32 [2048, 1024], P('fs', 'tp'), may hold values from -0.125 to 0.125
- out_w: float32 [1024, 2048], P('tp', 'fs'), may hold values from -0.1875 to 0.1875
- query_factor: bfloat16 [2048, 512], P('fs'), may hold values from -0.125 to 0.125
- out_factor: bfloat16 [2048, 512], P('fs'), may hold values from -0.125 to 0.125
- first_q: float32 [512, 1024], P('fs', 'tp'), may hold values from -6 to 6
- second_q: float32 [512, 1024], P('fs', 'tp'), may hold values from 0.075 to 120
- first_o: float32 [512, 1024], P('fs', 'tp'), may hold values from -6 to 6
- second_o: float32 [512, 1024], P('fs', 'tp'), may hold values from 0.075 to 120
Outputs:
- new_query_w: float32 [2048, 1024], P('fs', 'tp')
- new_out_w: float32 [1024, 2048], P('tp', 'fs')
- query_step: float32 [2048, 1024], P('fs', 'tp')
- out_step: float32 [1024, 2048], P('tp', 'fs')
- new_first_q: float32 [512, 1024], P('fs', 'tp')
- new_second_q: float32 [512, 1024], P('fs', 'tp')
- new_first_o: float32 [512, 1024], P('fs', 'tp')
- new_second_o: float32 [512, 1024], P('fs', 'tp')
- query_copy: bfloat16 [2048, 1024], P(None, 'tp')
- out_copy: bfloat16 [1024, 2048], P('tp')
The draws below stay inside these ranges and needn't reach their ends.
All inputs are finite; a program needn't handle non-finite values.
Results may differ from the reference program's by a relative error of at most 0.0085.
Values may be sent and summed in bfloat16 or wider, within the bound.
A program may use at most 64 MiB of HBM per device.

```python
import math
import jax
import jax.numpy as jnp
from jax import lax

D = 2048
RANK = 512
HQ = 1024
TOKENS = 12288


def second_law(key, marker):
    local_key = jax.random.fold_in(key, marker)
    row_place = jnp.arange(RANK, dtype=jnp.float32)[:, None] / RANK
    spread = jax.random.uniform(local_key, (RANK, HQ), jnp.float32, math.log(0.3), math.log(3.0))
    return jnp.exp(spread + row_place * math.log(10.0))


def draw_second_q(key, part):
    return second_law(key, 11)


def draw_second_o(key, part):
    return second_law(key, 23)


def raised(values, stream_key, source, target, shards_of, factor):
    def block_of(position):
        return (jnp.arange(values.shape[position]) // (values.shape[position] // shards_of)).reshape((-1,) + (1,) * (values.ndim - 1 - position))

    near = jax.random.permutation(stream_key, shards_of)[block_of(target)]
    far = (block_of(target) + shards_of // 2) % shards_of
    return jnp.where((block_of(source) == near) | (block_of(source) == far), factor * values, values)


def level_of(own_key, shape, shards, least, high):
    factor_of, own = 1.0, jax.random.fold_in(own_key, 6)
    for position, parts in shards:
        steps = jnp.exp(jax.random.uniform(jax.random.fold_in(own, position), (parts,), jnp.float32, least / len(shards), high / len(shards)))
        factor_of = factor_of * jnp.repeat(steps, shape[position] // parts).reshape([-1 if axis == position else 1 for axis in range(len(shape))])
    return factor_of


def normal_values(own_key, extent, width, reach, cuts=(), kind=jnp.bfloat16):
    values = jax.random.normal(own_key, extent, jnp.float32) * width
    if len(cuts) > 0:
        values = level_of(own_key, extent, cuts, -0.22, 0.18) * values
    return jnp.clip(values, min=-reach, max=reach).astype(kind)


def gaussian_with(stream_key, dims, width, bound, shards, heavy, kind=jnp.bfloat16):
    values = width * jax.random.normal(stream_key, dims, jnp.float32)
    if shards:
        values = values * level_of(stream_key, dims, shards, -0.22, 0.18)
    return jnp.clip(raised(values, jax.random.fold_in(stream_key, 3), *heavy), -bound, bound).astype(kind)


def setup_inputs(seed: int = 0) -> dict:
    key_of = jax.random.split(jax.random.key(seed), 13)
    input_act = gaussian_with(key_of[0], (TOKENS, D), 1.0, 6.0, ((0, 16),), (0, 1, 16, 2.0))
    query_cot = normal_values(key_of[1], (TOKENS, HQ), 1.0, 6.0, ((0, 16), (1, 2)))
    out_cot = gaussian_with(key_of[2], (TOKENS, D), 1.0, 6.0, ((0, 16),), (0, 1, 16, 2.0))
    attn_out = normal_values(key_of[3], (TOKENS, HQ), 1.0, 6.0, ((0, 16), (1, 2)))
    query_w = normal_values(key_of[4], (D, HQ), D ** -0.5, 0.125, ((0, 4), (1, 2)), jnp.float32)
    out_w = normal_values(key_of[5], (HQ, D), HQ ** -0.5, 0.1875, ((0, 2), (1, 4)), jnp.float32)
    query_factor = normal_values(key_of[6], (D, RANK), D ** -0.5, 0.125, ((0, 4),))
    out_factor = normal_values(key_of[7], (D, RANK), D ** -0.5, 0.125, ((0, 4),))
    first_q = normal_values(key_of[8], (RANK, HQ), 1.0, 6.0, ((0, 4), (1, 2)), jnp.float32)
    second_q = draw_second_q(jax.random.fold_in(key_of[12], 71), 0)
    first_o = normal_values(key_of[10], (RANK, HQ), 1.0, 6.0, ((0, 4), (1, 2)), jnp.float32)
    second_o = draw_second_o(jax.random.fold_in(key_of[12], 71), 0)
    return dict(input_act=input_act, query_cot=query_cot, out_cot=out_cot, attn_out=attn_out, query_w=query_w, out_w=out_w, query_factor=query_factor, out_factor=out_factor, first_q=first_q, second_q=second_q, first_o=first_o, second_o=second_o)


def contract_rows(left_side, right_side):
    return lax.dot_general(left_side, right_side, (((0,), (0,)), ((), ())), preferred_element_type=jnp.float32)

def exact_dot(left_side, right_side):
    return jnp.dot(left_side, right_side, precision=lax.Precision.HIGHEST, preferred_element_type=jnp.float32)

def reference(input_act, query_cot, out_cot, attn_out, query_w, out_w, query_factor, out_factor, first_q, second_q, first_o, second_o):
    scale_tokens = 1.0 / math.sqrt(TOKENS)
    grad_q = contract_rows(input_act, query_cot) * scale_tokens
    grad_o = contract_rows(out_cot, attn_out) * scale_tokens
    factor_q = query_factor.astype(jnp.float32)
    factor_o = out_factor.astype(jnp.float32)
    proj_q = exact_dot(factor_q.T, grad_q)
    proj_o = exact_dot(factor_o.T, grad_o)
    new_first_q = 0.8 * first_q + 0.2 * proj_q
    new_second_q = 0.9 * second_q + 0.1 * proj_q * proj_q
    new_first_o = 0.8 * first_o + 0.2 * proj_o
    new_second_o = 0.9 * second_o + 0.1 * proj_o * proj_o
    dir_q = new_first_q / jnp.sqrt(new_second_q)
    dir_o = new_first_o / jnp.sqrt(new_second_o)
    mean_square = (jnp.sum(dir_q * dir_q) + jnp.sum(dir_o * dir_o)) / (2 * RANK * HQ)
    norm_scale = jnp.sqrt(mean_square + 1e-06)
    query_step = exact_dot(factor_q, dir_q) / norm_scale
    out_step = (exact_dot(factor_o, dir_o) / norm_scale).T
    new_query_w = query_w - 0.01 * query_step
    new_out_w = out_w - 0.01 * out_step
    query_copy = new_query_w.astype(jnp.bfloat16)
    out_copy = new_out_w.astype(jnp.bfloat16)
    return (new_query_w, new_out_w, query_step, out_step, new_first_q, new_second_q, new_first_o, new_second_o, query_copy, out_copy)
```

```python
import functools
import math

import jax
import jax.numpy as jnp
from jax import lax
from jax.experimental import pallas as pl
from jax.experimental.pallas import tpu as pltpu
from jax.sharding import PartitionSpec as P

MESH = pl.DeviceIdType.MESH
F32 = jnp.float32
BF16 = jnp.bfloat16


def rcopy(src, dst, sems, index, there, **where):
    return pltpu.make_async_remote_copy(
        src_ref=src,
        dst_ref=dst,
        send_sem=sems[0].at[index],
        recv_sem=sems[1].at[there],
        device_id=where,
        device_id_type=MESH,
    )


def nt_dot(a, b):
    return lax.dot_general(a, b, (((1,), (1,)), ((), ())), preferred_element_type=F32)


def exchange_kernel(
    nf, nr, scale,
    x_ref, cq_ref, y_ref, ca_ref, wq_ref, wo_ref, fq_ref, fo_ref, m1q_ref, m2q_ref, m1o_ref, m2o_ref,
    fall_out, wq_out, wo_out, dir_out, proj_out, sq_out,
    acts, cots, cot_t, grads, fall, w32q, w32o, wbq, wbo, pieces, piece_in, summed, summed_in,
    moms, proj_all, dir_all, sq_all,
    loc, fa_s, fa_r, fb_s, fb_r, fc_s, fc_r, wz_s, wz_r, wx_s, wx_r, ps_s, ps_r, ss_s, ss_r,
    pr_s, pr_r, da_s, da_r, db_s, db_r, sq_s, sq_r,
):
    f, r, t = lax.axis_index("fs"), lax.axis_index("rep"), lax.axis_index("tp")
    ot = 1 - t
    dl, rank = fq_ref.shape
    hl = cq_ref.shape[1]
    dq, ch, pc, rl = dl // nr, rank // 2, hl // nr, rank // nf
    dh, hh = dl // 2, hl // 2
    fa, fb, fc = (fa_s, fa_r), (fb_s, fb_r), (fc_s, fc_r)
    wz, wx = (wz_s, wz_r), (wx_s, wx_r)
    ps, ss, pr, da, db, sq = (ps_s, ps_r), (ss_s, ss_r), (pr_s, pr_r), (da_s, da_r), (db_s, db_r), (sq_s, sq_r)

    def fpeer(k):
        return lax.rem(f + k, nf)

    def rpeer(j):
        return lax.rem(r + j, nr)

    def each_f(body, first=1, last=nf):
        lax.fori_loop(first, last, lambda k, _: (body(k, fpeer(k)), 0)[1], 0)

    def rows(start, size):
        return pl.ds(pl.multiple_of(start, 16), size)

    def local(i, src, dst):
        return pltpu.make_async_copy(src, dst, loc.at[i])

    own_rows = rows(f * dl, dl)
    load_f = [local(0, fq_ref, fall.at[0, own_rows]), local(1, fo_ref, fall.at[1, own_rows])]
    load_w = [local(2, wq_ref, w32q), local(3, wo_ref, w32o)]
    load_c = [local(4, cq_ref, cots.at[0]), local(5, ca_ref, cots.at[1])]
    load_x = [local(6, x_ref, acts.at[0]), local(7, y_ref, acts.at[1])]
    pcol = pl.ds(pl.multiple_of(r * pc, pc), pc)
    load_m = [
        local(8 + n, ref.at[:, pcol], moms.at[n])
        for n, ref in enumerate((m1q_ref, m2q_ref, m1o_ref, m2o_ref))
    ]
    for c in load_f + load_w + [load_c[0], load_x[0], load_c[1], load_x[1]] + load_m:
        c.start()

    barrier = pltpu.get_barrier_semaphore()
    each_f(lambda k, p: pl.semaphore_signal(barrier, inc=1, device_id={"fs": p}, device_id_type=MESH))
    for j in range(1, nr):
        pl.semaphore_signal(barrier, inc=1, device_id={"rep": rpeer(j)}, device_id_type=MESH)
    for j in range(nr):
        pl.semaphore_signal(barrier, inc=1, device_id={"rep": rpeer(j), "tp": ot}, device_id_type=MESH)
    pl.semaphore_wait(barrier, nf - 1 + 2 * nr - 1)

    def fcols(core):
        return pl.ds(pl.multiple_of(core * ch, ch), ch)

    def fchunk(i, core, block, part):
        return fall.at[i, rows(block * dl + part * dq, dq), fcols(core)]

    def fa_copy(i, p):
        return rcopy(fchunk(i, t, f, r), fchunk(i, t, f, r), fa, (i, p), (i, f), fs=p)

    def fb_copy(i, p, j):
        q = rpeer(j)
        return rcopy(fchunk(i, t, p, r), fchunk(i, t, p, r), fb, (i, p, q), (i, p, r), rep=q)

    def fc_copy(i, core, p):
        block = fall.at[i, rows(p * dl, dl), fcols(core)]
        return rcopy(block, block, fc, (i, p), (i, p), tp=ot)

    half = (lax.rem(r, 2), r // (nr // 2))
    mate = (r + 1 - 2 * half[0], lax.rem(r + nr // 2, nr))

    def w_piece(p, j, h):
        return wq_out.at[rows(p * dl + h * dh, dh)] if j == 0 else wo_out.at[p, rows(h * hh, hh)]

    def wz_copy(p, j, up):
        piece = w_piece(p, j, half[j])
        return rcopy(piece, piece, wz, (p, j, up), (p, j), fs=f + 1 if up else f - 1)

    def wz_own(j, up):
        own = (wbq.at[rows(half[0] * dh, dh)], wbo.at[rows(half[1] * hh, hh)])[j]
        return rcopy(own, w_piece(f, j, half[j]), wz, (f, j, up), (f, j), fs=f + 1 if up else f - 1)

    def wx_copy(p, j):
        piece = w_piece(p, j, half[j])
        return rcopy(piece, piece, wx, (p, j), (p, j), rep=mate[j])

    def wx_recv(p, j):
        piece = w_piece(p, j, 1 - half[j])
        return rcopy(piece, piece, wx, (p, j), (p, j), rep=mate[j])

    def w_ends(act):
        for up in (0, 1):
            @pl.when(f < nf - 1 if up else f > 0)
            def _():
                act(up)

    def w_lines(k, act):
        for up in (0, 1):
            p = f - k if up else f + k

            @pl.when(p >= 0 if up else p < nf)
            def _():
                act(p, up)

    def w_step(k, j):
        def act(p, up):
            wz_copy(p, j, up).wait_recv()

            @pl.when(f < nf - 1 if up else f > 0)
            def _():
                wz_copy(p, j, up).start()

            wx_copy(p, j).start()

        w_lines(k, act)

    for c in load_f:
        c.wait()
    for i in range(2):
        each_f(lambda k, p: fa_copy(i, p).start())

    for c in load_w:
        c.wait()
    wbq[...] = w32q[...].astype(BF16)
    wbo[...] = w32o[...].astype(BF16)
    keep_w = [local(2, wbq, wq_out.at[own_rows]), local(3, wbo, wo_out.at[f])]
    for c in keep_w:
        c.start()
    for j in range(2):
        w_ends(lambda up: wz_own(j, up).start())

    nb = min(512, x_ref.shape[1])

    def gradient(i):
        load_c[i].wait()
        cot_t[...] = cots[i].T
        load_x[i].wait()

        def column(n, _):
            cols = pl.ds(pl.multiple_of(n * nb, nb), nb)
            grads[i, :, cols] = jnp.dot(cot_t[...], acts[i, :, cols], preferred_element_type=F32).astype(BF16)
            return 0

        lax.fori_loop(0, x_ref.shape[1] // nb, column, 0)

    def forward_f(i, first, last):
        def step(k, p):
            rcopy(fchunk(i, t, p, r), fchunk(i, t, p, r), fa, (i, p), (i, p), fs=p).wait_recv()
            for j in range(1, nr):
                fb_copy(i, p, j).start()

        each_f(step, first, last)

    def across_f(i):
        def step(k, p):
            for j in range(1, nr):
                q = rpeer(j)
                rcopy(fchunk(i, t, p, q), fchunk(i, t, p, q), fb, (i, p, q), (i, p, q), rep=q).wait_recv()
            fc_copy(i, t, p).start()

        each_f(step)
        each_f(lambda k, p: fc_copy(i, ot, p).wait_recv())

    rb = min(256, rank)

    def ps_copy(i, j):
        q = rpeer(j)
        return rcopy(pieces.at[i, q], piece_in.at[i, r], ps, (i, q), (i, r), rep=q)

    def project(i):
        def ranks(n, _):
            cols = pl.ds(pl.multiple_of(n * rb, rb), rb)
            term = jnp.dot(grads[i], fall[i, :, cols], preferred_element_type=F32).T.astype(BF16)
            for part in range(nr):
                pieces[i, part, cols, :] = term[:, part * pc:(part + 1) * pc]
            return 0

        lax.fori_loop(0, rank // rb, ranks, 0)
        for j in range(1, nr):
            ps_copy(i, j).start()

    def ss_copy(i, p):
        return rcopy(summed.at[i, rows(p * rl, rl)], summed_in.at[i, f], ss, (i, p), (i, f), fs=p)

    def reduce_rep(i):
        for j in range(1, nr):
            q = rpeer(j)
            rcopy(pieces.at[i, q], piece_in.at[i, q], ps, (i, q), (i, q), rep=q).wait_recv()
        total = pieces[i, r].astype(F32)
        for j in range(1, nr):
            total = total + piece_in[i, rpeer(j)].astype(F32)
        summed[i] = total.astype(BF16)
        each_f(lambda k, p: ss_copy(i, p).start())

    own_rank = rows(f * rl, rl)

    def pr_copy(i, j):
        q = rpeer(j)
        return rcopy(proj_all.at[i, r], proj_all.at[i, r], pr, (i, q), (i, r), rep=q)

    def da_copy(i, p):
        own = dir_all.at[i, r, own_rank]
        return rcopy(own, own, da, (i, p), (i, f), fs=p)

    def direction(i):
        def gather_sum(k, total):
            p = fpeer(k)
            rcopy(summed.at[i, own_rank], summed_in.at[i, p], ss, (i, p), (i, p), fs=p).wait_recv()
            return total + summed_in[i, p].astype(F32)

        proj = lax.fori_loop(1, nf, gather_sum, summed[i, own_rank, :].astype(F32)).astype(BF16)
        proj_all[i, r] = proj
        proj = proj.astype(F32) * scale
        load_m[2 * i].wait()
        load_m[2 * i + 1].wait()
        first = 0.8 * moms[2 * i] + 0.2 * proj
        second = 0.9 * moms[2 * i + 1] + 0.1 * proj * proj
        dir_all[i, r, own_rank, :] = (first / jnp.sqrt(second)).astype(BF16)
        each_f(lambda k, p: da_copy(i, p).start())
        for j in range(1, nr):
            pr_copy(i, j).start()

    def db_copy(i, j):
        q = rpeer(j)
        return rcopy(dir_all.at[i, r], dir_all.at[i, r], db, (i, q), (i, r), rep=q)

    def da_waits(i):
        def step(k, p):
            there = dir_all.at[i, r, rows(p * rl, rl)]
            rcopy(there, there, da, (i, p), (i, p), fs=p).wait_recv()

        each_f(step)

    def spread(i):
        for j in range(1, nr):
            db_copy(i, j).start()

    peers = [(j, c) for j in range(nr) for c in range(2) if j + c > 0]

    def sq_copy(j, c):
        q, core = rpeer(j), (t, ot)[c]
        return rcopy(sq_all.at[r, t], sq_all.at[r, t], sq, (q, core), (r, t), rep=q, tp=core)

    def sq_recv(j, c):
        q, core = rpeer(j), (t, ot)[c]
        return rcopy(sq_all.at[q, core], sq_all.at[q, core], sq, (q, core), (q, core), rep=q, tp=core)

    def squares():
        total = jnp.zeros((8, pc), F32)
        for i in range(2):
            d = dir_all[i, r].astype(F32)
            total = total + jnp.sum((d * d).reshape(rank // 8, 8, pc), axis=0)
        sq_all[r, t] = total
        for j, c in peers:
            sq_copy(j, c).start()

    def w_steps(first, last, js=(0, 1)):
        def step(k, _):
            for j in js:
                w_step(k, j)
            return 0

        lax.fori_loop(first, max(first, last), step, 0)

    early = 1 + (nf - 1) // 3
    forward_f(0, 1, early)
    gradient(0)
    forward_f(0, early, nf)
    gradient(1)
    forward_f(1, 1, nf)
    across_f(0)
    keep_f = [local(0, fall.at[0], fall_out.at[0]), local(1, fall.at[1], fall_out.at[1])]
    keep_f[0].start()
    project(0)
    across_f(1)
    keep_f[1].start()
    project(1)
    w_steps(1, min(2, nf))
    reduce_rep(0)
    reduce_rep(1)
    direction(0)
    direction(1)
    da_waits(0)
    spread(0)
    da_waits(1)
    squares()
    spread(1)
    w_steps(2, nf)

    def db_waits(i):
        for j in range(1, nr):
            q = rpeer(j)
            rcopy(dir_all.at[i, q], dir_all.at[i, q], db, (i, q), (i, q), rep=q).wait_recv()
            rcopy(proj_all.at[i, q], proj_all.at[i, q], pr, (i, q), (i, q), rep=q).wait_recv()

    for i in range(2):
        db_waits(i)
    keep_d = [local(4, dir_all, dir_out), local(5, proj_all, proj_out)]
    for c in keep_d:
        c.start()
    for j, c in peers:
        sq_recv(j, c).wait_recv()
    whole = jnp.zeros((8, pc), F32)
    for q in range(nr):
        for core in range(2):
            whole = whole + sq_all[q, core]
    sq_out[...] = jnp.zeros(sq_out.shape, F32) + jnp.sum(whole)

    def rest_w(k, p):
        for j in range(2):
            wx_recv(p, j).wait_recv()

    each_f(rest_w)

    def drain(k, p):
        for i in range(2):
            fa_copy(i, p).wait_send()
            for j in range(1, nr):
                fb_copy(i, p, j).wait_send()
            fc_copy(i, t, p).wait_send()
            ss_copy(i, p).wait_send()
            da_copy(i, p).wait_send()
            wx_copy(p, i).wait_send()

            def act(p, up):
                @pl.when(f < nf - 1 if up else f > 0)
                def _():
                    wz_copy(p, i, up).wait_send()

            w_lines(k, act)

    each_f(drain)
    for i in range(2):
        w_ends(lambda up: wz_own(i, up).wait_send())
        for j in range(1, nr):
            ps_copy(i, j).wait_send()
            pr_copy(i, j).wait_send()
            db_copy(i, j).wait_send()
    for j, c in peers:
        sq_copy(j, c).wait_send()
    for c in keep_w + keep_f + keep_d:
        c.wait()


def apply_kernel(
    nr, count, scale,
    fall_ref, wq_ref, wo_ref, dir_ref, proj_ref, sq_ref, w32q_ref, w32o_ref, fq_ref, fo_ref,
    m1q_ref, m2q_ref, m1o_ref, m2o_ref,
    nwq_ref, nwo_ref, sq_out, so_out, n1q_ref, n2q_ref, n1o_ref, n2o_ref, cq_ref, co_ref,
    dirs,
):
    inverse = 1.0 / jnp.sqrt(sq_ref[0:1, 0:1] / count + 1e-06)

    @pl.when(pl.program_id(0) == 0)
    def _():
        dirs[0] = jnp.concatenate([dir_ref[0, q] for q in range(nr)], axis=1)
        dirs[1] = jnp.concatenate([dir_ref[1, q] for q in range(nr)], axis=1).T
        step_q = jnp.dot(fq_ref[...], dirs[0], preferred_element_type=F32) * inverse
        sq_out[...] = step_q
        nwq_ref[...] = w32q_ref[...] - 0.01 * step_q
        step_o = nt_dot(dirs[1], fo_ref[...]) * inverse
        so_out[...] = step_o
        nwo_ref[...] = w32o_ref[...] - 0.01 * step_o
        proj_q = jnp.concatenate([proj_ref[0, q] for q in range(nr)], axis=1).astype(F32) * scale
        proj_o = jnp.concatenate([proj_ref[1, q] for q in range(nr)], axis=1).astype(F32) * scale
        n1q_ref[...] = 0.8 * m1q_ref[...] + 0.2 * proj_q
        n2q_ref[...] = 0.9 * m2q_ref[...] + 0.1 * proj_q * proj_q
        n1o_ref[...] = 0.8 * m1o_ref[...] + 0.2 * proj_o
        n2o_ref[...] = 0.9 * m2o_ref[...] + 0.1 * proj_o * proj_o

    step_q = jnp.dot(fall_ref[0], dirs[0], preferred_element_type=F32) * inverse
    cq_ref[...] = (wq_ref[...].astype(F32) - 0.01 * step_q).astype(BF16)
    step_o = nt_dot(dirs[1], fall_ref[1]) * inverse
    whole_w = jnp.concatenate([wo_ref[m].astype(F32) for m in range(wo_ref.shape[0])], axis=1)
    co_ref[...] = (whole_w - 0.01 * step_o).astype(BF16)


def body(
    nf, nr,
    input_act, query_cot, out_cot, attn_out, query_w, out_w, query_factor, out_factor,
    first_q, second_q, first_o, second_o,
):
    tokens, d = input_act.shape
    hl = query_cot.shape[1]
    dl, rank = query_factor.shape
    rl = first_q.shape[0]
    pc = hl // nr
    scale = 1.0 / math.sqrt(tokens * nf * nr)
    anyspace = pl.BlockSpec(memory_space=pltpu.HBM)
    dma = pltpu.SemaphoreType.DMA
    sds = jax.ShapeDtypeStruct
    sems = []
    for send, recv in (
        ((2, nf), (2, nf)),
        ((2, nf, nr), (2, nf, nr)),
        ((2, nf), (2, nf)),
        ((nf, 2, 2), (nf, 2)),
        ((nf, 2), (nf, 2)),
        ((2, nr), (2, nr)),
        ((2, nf), (2, nf)),
        ((2, nr), (2, nr)),
        ((2, nf), (2, nf)),
        ((2, nr), (2, nr)),
        ((nr, 2), (nr, 2)),
    ):
        sems += [dma(send), dma(recv)]
    fall, wq_all, wo_all, dirs, projs, squares = pl.pallas_call(
        functools.partial(exchange_kernel, nf, nr, scale),
        out_shape=(
            sds((2, d, rank), BF16),
            sds((d, hl), BF16),
            sds((nf, hl, dl), BF16),
            sds((2, nr, rank, pc), BF16),
            sds((2, nr, rl, pc), BF16),
            sds((8, 128), F32),
        ),
        in_specs=[anyspace] * 12,
        out_specs=(anyspace,) * 5 + (pl.BlockSpec(memory_space=pltpu.VMEM),),
        scratch_shapes=[
            pltpu.VMEM((2, tokens, d), BF16),
            pltpu.VMEM((2, tokens, hl), BF16),
            pltpu.VMEM((hl, tokens), BF16),
            pltpu.VMEM((2, hl, d), BF16),
            pltpu.VMEM((2, d, rank), BF16),
            pltpu.VMEM((dl, hl), F32),
            pltpu.VMEM((hl, dl), F32),
            pltpu.VMEM((dl, hl), BF16),
            pltpu.VMEM((hl, dl), BF16),
            pltpu.VMEM((2, nr, rank, pc), BF16),
            pltpu.VMEM((2, nr, rank, pc), BF16),
            pltpu.VMEM((2, rank, pc), BF16),
            pltpu.VMEM((2, nf, rl, pc), BF16),
            pltpu.VMEM((4, rl, pc), F32),
            pltpu.VMEM((2, nr, rl, pc), BF16),
            pltpu.VMEM((2, nr, rank, pc), BF16),
            pltpu.VMEM((nr, 2, 8, pc), F32),
            dma((12,)),
        ] + sems,
        compiler_params=pltpu.CompilerParams(
            collective_id=0, has_side_effects=True, vmem_limit_bytes=67043328
        ),
    )(
        input_act, query_cot, out_cot, attn_out, query_w, out_w, query_factor, out_factor,
        first_q, second_q, first_o, second_o,
    )
    group = min(nf, max(1, 128 // dl))
    whole = lambda a: pl.BlockSpec(a.shape, lambda j, n=len(a.shape): (0,) * n)
    locals_in = (dirs, projs, squares, query_w, out_w, query_factor, out_factor, first_q, second_q, first_o, second_o)
    results = (query_w, out_w, query_w, out_w, first_q, second_q, first_o, second_o)
    outs = pl.pallas_call(
        functools.partial(apply_kernel, nr, 2 * rank * hl * 2, scale),
        grid=(nf // group,),
        out_shape=tuple(sds(a.shape, F32) for a in results) + (sds((d, hl), BF16), sds((hl, d), BF16)),
        in_specs=[
            pl.BlockSpec((2, group * dl, rank), lambda j: (0, j, 0)),
            pl.BlockSpec((group * dl, hl), lambda j: (j, 0)),
            pl.BlockSpec((group, hl, dl), lambda j: (j, 0, 0)),
        ] + [whole(a) for a in locals_in],
        out_specs=tuple(whole(a) for a in results) + (
            pl.BlockSpec((group * dl, hl), lambda j: (j, 0)),
            pl.BlockSpec((hl, group * dl), lambda j: (0, j)),
        ),
        scratch_shapes=[pltpu.VMEM((2, rank, hl), BF16)],
        compiler_params=pltpu.CompilerParams(vmem_limit_bytes=67043328),
    )(fall, wq_all, wo_all, *locals_in)
    return outs


def solution(mesh):
    return jax.shard_map(
        functools.partial(body, mesh.shape["fs"], mesh.shape["rep"]),
        mesh=mesh,
        in_specs=(
            P(("fs", "rep"), None),
            P(("fs", "rep"), "tp"),
            P(("fs", "rep"), None),
            P(("fs", "rep"), "tp"),
            P("fs", "tp"),
            P("tp", "fs"),
            P("fs", None),
            P("fs", None),
            P("fs", "tp"),
            P("fs", "tp"),
            P("fs", "tp"),
            P("fs", "tp"),
        ),
        out_specs=(
            P("fs", "tp"),
            P("tp", "fs"),
            P("fs", "tp"),
            P("tp", "fs"),
            P("fs", "tp"),
            P("fs", "tp"),
            P("fs", "tp"),
            P("fs", "tp"),
            P(None, "tp"),
            P("tp", None),
        ),
        check_vma=False,
    )
```

```python
import functools
import math

import jax
import jax.numpy as jnp
from jax import lax
from jax.experimental import pallas as pl
from jax.experimental.pallas import tpu as pltpu
from jax.sharding import PartitionSpec as P

MESH = pl.DeviceIdType.MESH
F32 = jnp.float32
BF16 = jnp.bfloat16
VMEM_LIMIT = 40 << 20


def rcopy(src, dst, sems, index, there, **where):
    return pltpu.make_async_remote_copy(
        src_ref=src,
        dst_ref=dst,
        send_sem=sems[0].at[index],
        recv_sem=sems[1].at[there],
        device_id=where,
        device_id_type=MESH,
    )


def nt_dot(a, b):
    return lax.dot_general(a, b, (((1,), (1,)), ((), ())), preferred_element_type=F32)


def exchange_kernel(
    nf, nr, scale,
    x_ref, cq_ref, y_ref, ca_ref, wq_ref, wo_ref, fq_ref, fo_ref, m1q_ref, m2q_ref, m1o_ref, m2o_ref,
    fall, wq_out, wo_out, dir_all, proj_all, sq_out, w32q, w32o, moms,
    acts, cots, cot_t, grads, pieces, piece_in, summed, summed_in, sq_all,
    loc, fa_s, fa_r, fb_s, fb_r, fc_s, fc_r, wz_s, wz_r, wx_s, wx_r, ps_s, ps_r, ss_s, ss_r,
    pr_s, pr_r, da_s, da_r, db_s, db_r, sq_s, sq_r,
):
    f, r, t = lax.axis_index("fs"), lax.axis_index("rep"), lax.axis_index("tp")
    ot = 1 - t
    dl, rank = fq_ref.shape
    hl = cq_ref.shape[1]
    dq, ch, pc, rl = dl // nr, rank // 2, hl // nr, rank // nf
    dh, hh = dl // 2, hl // 2
    fa, fb, fc = (fa_s, fa_r), (fb_s, fb_r), (fc_s, fc_r)
    wz, wx = (wz_s, wz_r), (wx_s, wx_r)
    ps, ss, pr, da, db, sq = (ps_s, ps_r), (ss_s, ss_r), (pr_s, pr_r), (da_s, da_r), (db_s, db_r), (sq_s, sq_r)

    def fpeer(k):
        return lax.rem(f + k, nf)

    def rpeer(j):
        return lax.rem(r + j, nr)

    def each_f(body):
        lax.fori_loop(1, nf, lambda k, _: (body(fpeer(k)), 0)[1], 0)

    def rows(start, size):
        return pl.ds(pl.multiple_of(start, 16), size)

    def pcols(part):
        return pl.ds(pl.multiple_of(part * pc, pc), pc)

    def local(i, src, dst):
        return pltpu.make_async_copy(src, dst, loc.at[i])

    own_rows = rows(f * dl, dl)
    load_f = [local(0, fq_ref, fall.at[0, own_rows]), local(1, fo_ref, fall.at[1, own_rows])]
    load_w = [local(2, wq_ref, w32q), local(3, wo_ref, w32o)]
    load_c = [local(4, cq_ref, cots.at[0]), local(5, ca_ref, cots.at[1])]
    load_x = [local(6, x_ref, acts.at[0]), local(7, y_ref, acts.at[1])]
    load_m = [local(8 + n, ref, moms.at[n]) for n, ref in enumerate((m1q_ref, m2q_ref, m1o_ref, m2o_ref))]
    for c in load_f + load_w + [load_c[0], load_x[0], load_c[1], load_x[1]] + load_m:
        c.start()

    barrier = pltpu.get_barrier_semaphore()
    each_f(lambda p: pl.semaphore_signal(barrier, inc=1, device_id={"fs": p}, device_id_type=MESH))
    for j in range(1, nr):
        pl.semaphore_signal(barrier, inc=1, device_id={"rep": rpeer(j)}, device_id_type=MESH)
    for j in range(nr):
        pl.semaphore_signal(barrier, inc=1, device_id={"rep": rpeer(j), "tp": ot}, device_id_type=MESH)
    pl.semaphore_wait(barrier, nf - 1 + 2 * nr - 1)

    def line(k, act):
        for up in (0, 1):
            p = f - k if up else f + k

            @pl.when(p >= 0 if up else p < nf)
            def _():
                act(p, up)

    def each_line(act):
        lax.fori_loop(1, nf, lambda k, _: (line(k, lambda p, up: act(p)), 0)[1], 0)

    def onward(up):
        return f < nf - 1 if up else f > 0

    half = (lax.rem(r, 2), r // (nr // 2))
    mate = (r + 1 - 2 * half[0], lax.rem(r + nr // 2, nr))

    def hops(i):
        return ((r, mate[i], 0), (r, mate[1 - i], 1), (mate[i], mate[1 - i], 1))

    def fcols(core):
        return pl.ds(pl.multiple_of(core * ch, ch), ch)

    def fchunk(i, core, block, part, count=1):
        return fall.at[i, rows(block * dl + part * dq, count * dq), fcols(core)]

    def fa_copy(i, p):
        return rcopy(fchunk(i, t, f, r), fchunk(i, t, f, r), fa, 0, (i, f), fs=p)

    def fb_copy(i, p, n):
        part, to, slot = hops(i)[n]
        return rcopy(fchunk(i, t, p, part), fchunk(i, t, p, part), fb, 0, (i, p, slot), rep=to)

    def fb_wait(i, p, slot):
        there = fchunk(i, t, p, 0, 1 + slot)
        rcopy(there, there, fb, 0, (i, p, slot), rep=mate[0]).wait_recv()

    def fc_copy(i, core, p):
        block = fall.at[i, rows(p * dl, dl), fcols(core)]
        return rcopy(block, block, fc, 0, (i, p), tp=ot)

    def arrive_f(i, p):
        rcopy(fchunk(i, t, p, r), fchunk(i, t, p, r), fa, 0, (i, p), fs=p).wait_recv()
        for n in range(2):
            fb_copy(i, p, n).start()

    def relay_f(i, p):
        fb_wait(i, p, 0)
        fb_copy(i, p, 2).start()

    def across_f(i, p):
        fb_wait(i, p, 1)
        fc_copy(i, t, p).start()

    def rest_f(i):
        each_line(lambda p: fc_copy(i, ot, p).wait_recv())

    def w_piece(p, j, h):
        size = (dh, hh)[j % 2]
        start = h * size + j // 2 * (size // 2)
        if j % 2 == 0:
            return wq_out.at[rows(p * dl + start, size // 2)]
        return wo_out.at[p, rows(start, size // 2)]

    def wz_copy(p, j, up):
        piece = w_piece(p, j, half[j % 2])
        return rcopy(piece, piece, wz, (p, up), (p, j), fs=f + 1 if up else f - 1)

    def wx_copy(p, j):
        piece = w_piece(p, j, half[j % 2])
        return rcopy(piece, piece, wx, 0, 0, rep=mate[j % 2])

    def w_step(k, i, wait=True, ahead=True, plane=True):
        for j in (i, i + 2):
            def act(p, up):
                if wait:
                    wz_copy(p, j, up).wait_recv()
                if ahead:
                    pl.when(onward(up))(lambda: wz_copy(p, j, up).start())
                if plane:
                    wx_copy(p, j).start()

            line(k, act)

    for c in load_f:
        c.wait()
    for i in range(2):
        each_line(lambda p: fa_copy(i, p).start())

    for c in load_w:
        c.wait()
    wq_out[own_rows, :] = w32q[...].astype(BF16)
    wo_out[f] = w32o[...].astype(BF16)
    for j in (0, 2, 1, 3):
        for up in (0, 1):
            pl.when(onward(up))(lambda: wz_copy(f, j, up).start())

    nb = min(512, x_ref.shape[1])

    def gradient(i):
        load_c[i].wait()
        cot_t[...] = cots[i].T
        load_x[i].wait()

        def column(n, _):
            cols = pl.ds(pl.multiple_of(n * nb, nb), nb)
            grads[i, :, cols] = jnp.dot(cot_t[...], acts[i, :, cols], preferred_element_type=F32).astype(BF16)
            return 0

        lax.fori_loop(0, x_ref.shape[1] // nb, column, 0)

    rb = min(256, rank)

    def ps_copy(i, j):
        q = rpeer(j)
        return rcopy(pieces.at[i, q], piece_in.at[i, r], ps, 0, i, rep=q)

    def project(i):
        def ranks(n, _):
            cols = pl.ds(pl.multiple_of(n * rb, rb), rb)
            term = jnp.dot(grads[i], fall[i, :, cols], preferred_element_type=F32).T.astype(BF16)
            for part in range(nr):
                pieces[i, part, cols, :] = term[:, part * pc:(part + 1) * pc]
            return 0

        lax.fori_loop(0, rank // rb, ranks, 0)
        for j in range(1, nr):
            ps_copy(i, j).start()

    def ss_copy(i, p):
        return rcopy(summed.at[i, rows(p * rl, rl)], summed_in.at[i, f], ss, 0, i, fs=p)

    def reduce_rep(i):
        there = piece_in.at[i, pl.ds(0, nr - 1)]
        rcopy(there, there, ps, 0, i, rep=mate[0]).wait_recv()
        total = pieces[i, r].astype(F32)
        for j in range(1, nr):
            total = total + piece_in[i, rpeer(j)].astype(F32)
        summed[i] = total.astype(BF16)
        each_f(lambda p: ss_copy(i, p).start())

    own_rank = rows(f * rl, rl)

    def pr_copy(i, j):
        own = proj_all.at[i, :, pcols(r)]
        return rcopy(own, own, pr, 0, 0, rep=rpeer(j))

    def da_copy(i, p):
        own = dir_all.at[i, own_rank, pcols(r)]
        return rcopy(own, own, da, 0, i, fs=p)

    def direction(i):
        there = summed_in.at[i, pl.ds(0, nf - 1)]
        rcopy(there, there, ss, 0, i, fs=fpeer(1)).wait_recv()

        def gather_sum(k, total):
            return total + summed_in[i, fpeer(k)].astype(F32)

        proj = lax.fori_loop(1, nf, gather_sum, summed[i, own_rank, :].astype(F32)).astype(BF16)
        proj_all[i, :, pcols(r)] = proj
        proj = proj.astype(F32) * scale
        load_m[2 * i].wait()
        load_m[2 * i + 1].wait()
        first = 0.8 * moms[2 * i, :, pcols(r)] + 0.2 * proj
        second = 0.9 * moms[2 * i + 1, :, pcols(r)] + 0.1 * proj * proj
        dir_all[i, own_rank, pcols(r)] = (first / jnp.sqrt(second)).astype(BF16)
        each_f(lambda p: da_copy(i, p).start())
        for j in range(1, nr):
            pr_copy(i, j).start()

    def da_waits(i):
        there = dir_all.at[i, pl.ds(0, (nf - 1) * rl), pl.ds(0, pc)]
        rcopy(there, there, da, 0, i, fs=fpeer(1)).wait_recv()

    def db_copy(i, n):
        part, to, slot = hops(i)[n]
        piece = dir_all.at[i, :, pcols(part)]
        return rcopy(piece, piece, db, 0, (i, slot), rep=to)

    def db_wait(i, slot):
        there = dir_all.at[i, :, pl.ds(0, (1 + slot) * pc)]
        rcopy(there, there, db, 0, (i, slot), rep=mate[0]).wait_recv()

    def spread(i):
        for n in range(2):
            db_copy(i, n).start()

    def spread_on(i):
        db_wait(i, 0)
        db_copy(i, 2).start()

    peers = [(j, c) for j in range(nr) for c in range(2) if j + c > 0]

    def sq_copy(j, c):
        own = sq_all.at[2 * r + t]
        return rcopy(own, own, sq, 0, 0, rep=rpeer(j), tp=(t, ot)[c])

    def squares():
        total = jnp.zeros((8, pc), F32)
        for i in range(2):
            d = dir_all[i, :, pcols(r)].astype(F32)
            total = total + jnp.sum((d * d).reshape(rank // 8, 8, pc), axis=0)
        sq_all[2 * r + t] = total
        for j, c in peers:
            sq_copy(j, c).start()

    inner = jnp.logical_and(f > 0, f < nf - 1)

    def forward_f():
        def step(p):
            relay_f(0, p)
            arrive_f(1, p)

        each_line(step)

    def finish_f():
        def step(p):
            across_f(0, p)
            relay_f(1, p)

        each_line(step)

    gradient(0)
    each_line(lambda p: arrive_f(0, p))
    gradient(1)
    forward_f()
    finish_f()
    rest_f(0)
    project(0)
    w_step(1, 0, plane=False)
    each_line(lambda p: across_f(1, p))
    rest_f(1)
    project(1)
    w_step(1, 0, wait=False, ahead=False)
    w_step(1, 1, ahead=False)
    reduce_rep(0)
    w_step(1, 1, wait=False, plane=False)
    reduce_rep(1)
    pl.when(~inner)(lambda: w_step(2, 0, ahead=False))
    direction(0)
    pl.when(~inner)(lambda: w_step(2, 1, ahead=False))
    direction(1)
    pl.when(~inner)(lambda: w_step(2, 0, wait=False, plane=False))
    pl.when(~inner)(lambda: w_step(2, 1, wait=False, plane=False))
    pl.when(inner)(lambda: w_step(2, 0, plane=False))
    pl.when(inner)(lambda: w_step(2, 1, plane=False))
    da_waits(0)
    spread(0)
    da_waits(1)
    squares()
    spread(1)
    spread_on(0)
    spread_on(1)
    pl.when(inner)(lambda: w_step(2, 0, wait=False, ahead=False))
    pl.when(inner)(lambda: w_step(2, 1, wait=False, ahead=False))

    def w_steps(k, _):
        for i in range(2):
            w_step(k, i)
        return 0

    lax.fori_loop(3, max(3, nf), w_steps, 0)

    def finish():
        for i in range(2):
            db_wait(i, 1)
        there = sq_all.at[pl.ds(0, 2 * nr - 1)]
        rcopy(there, there, sq, 0, 0, tp=ot).wait()
        total = sq_all[0]
        for n in range(1, 2 * nr):
            total = total + sq_all[n]
        sq_out[...] = jnp.zeros(sq_out.shape, F32) + jnp.sum(total)
        there = proj_all.at[:, :, pl.ds(0, (nr - 1) * pc)]
        rcopy(there, there, pr, 0, 0, rep=mate[0]).wait()

    finish()

    def rest_w():
        there = wq_out.at[pl.ds(0, (nf - 1) * dl)]
        rcopy(there, there, wx, 0, 0, rep=mate[0]).wait()

    rest_w()

    def drain():
        def blocks(p, _):
            for up in (0, 1):
                sent = wq_out.at[rows(p * dl, dl)]
                pl.when(jnp.logical_and(onward(up), p <= f if up else p >= f))(
                    lambda: rcopy(sent, sent, wz, (p, up), (p, 0), fs=fpeer(1)).wait_send()
                )
            return 0

        lax.fori_loop(0, nf, blocks, 0)
        for sent, sems in (
            (fall.at[:, pl.ds(0, (nf - 1) * dq), fcols(0)], fa),
            (fall.at[:, pl.ds(0, 3 * (nf - 1) * dq), fcols(0)], fb),
            (fall.at[:, pl.ds(0, (nf - 1) * dl), fcols(0)], fc),
            (pieces.at[:, pl.ds(0, nr - 1)], ps),
            (summed.at[:, pl.ds(0, (nf - 1) * rl)], ss),
            (dir_all.at[:, pl.ds(0, (nf - 1) * rl), pl.ds(0, pc)], da),
            (dir_all.at[:, :, pl.ds(0, 3 * pc)], db),
        ):
            rcopy(sent, sent, (sems[0], sems[0]), 0, 0, tp=ot).wait_send()

    drain()


def apply_kernel(
    nf, nr, group, count, scale,
    fall, wq, wo, dir_ref, proj, sq_ref, w32q, w32o, moms,
    nwq_out, nwo_out, sq_out, so_out, n1q_out, n2q_out, n1o_out, n2o_out, cq_out, co_out,
    dir_t, stage_q, stage_o, stage_m, copy_q, copy_o, sems,
):
    f = lax.axis_index("fs")
    dl, hl = w32q.shape
    inverse = 1.0 / jnp.sqrt(sq_ref[0:1, 0:1] / count + 1e-06)

    def out(i, src, dst):
        copy = pltpu.make_async_copy(src, dst, sems.at[i])
        copy.start()
        return copy

    sent = []
    for i, (first_out, second_out) in enumerate(((n1q_out, n2q_out), (n1o_out, n2o_out))):
        scaled = proj[i].astype(F32) * scale
        stage_m[2 * i] = 0.8 * moms[2 * i] + 0.2 * scaled
        stage_m[2 * i + 1] = 0.9 * moms[2 * i + 1] + 0.1 * scaled * scaled
        sent += [out(2 * i, stage_m.at[2 * i], first_out), out(2 * i + 1, stage_m.at[2 * i + 1], second_out)]

    own = pl.ds(pl.multiple_of(f * dl, dl), dl)
    step_q = jnp.dot(fall[0, own, :], dir_ref[0], preferred_element_type=F32) * inverse
    stage_q[0] = step_q
    sent += [out(4, stage_q.at[0], sq_out)]
    stage_q[1] = w32q[...] - 0.01 * step_q
    sent += [out(5, stage_q.at[1], nwq_out)]
    dir_t[...] = dir_ref[1].T
    step_o = nt_dot(dir_t[...], fall[1, own, :]) * inverse
    stage_o[0] = step_o
    sent += [out(6, stage_o.at[0], so_out)]
    stage_o[1] = w32o[...] - 0.01 * step_o
    sent += [out(7, stage_o.at[1], nwo_out)]

    size = group * dl

    def block(g, _):
        part = pl.ds(pl.multiple_of(g * size, size), size)
        step_q = jnp.dot(fall[0, part, :], dir_ref[0], preferred_element_type=F32) * inverse
        copy_q[part, :] = (wq[part, :].astype(F32) - 0.01 * step_q).astype(BF16)
        pltpu.make_async_copy(copy_q.at[part], cq_out.at[part], sems.at[8]).start()
        step_o = nt_dot(dir_t[...], fall[1, part, :]) * inverse
        weight = jnp.concatenate([wo[g * group + m] for m in range(group)], axis=1).astype(F32)
        copy_o[:, part] = (weight - 0.01 * step_o).astype(BF16)
        pltpu.make_async_copy(copy_o.at[:, part], co_out.at[:, part], sems.at[9]).start()
        return 0

    lax.fori_loop(0, nf // group, block, 0)
    pltpu.make_async_copy(copy_q, cq_out, sems.at[8]).wait()
    pltpu.make_async_copy(copy_o, co_out, sems.at[9]).wait()
    for copy in sent:
        copy.wait()


def body(
    nf, nr,
    input_act, query_cot, out_cot, attn_out, query_w, out_w, query_factor, out_factor,
    first_q, second_q, first_o, second_o,
):
    tokens, d = input_act.shape
    hl = query_cot.shape[1]
    dl, rank = query_factor.shape
    rl = first_q.shape[0]
    pc = hl // nr
    scale = 1.0 / math.sqrt(tokens * nf * nr)
    hbm = pl.BlockSpec(memory_space=pltpu.HBM)
    vmem = pl.BlockSpec(memory_space=pltpu.VMEM)
    dma = pltpu.SemaphoreType.DMA
    sds = jax.ShapeDtypeStruct
    one = (1,)
    sems = []
    for send, recv in (
        (one, (2, nf)),
        (one, (2, nf, 2)),
        (one, (2, nf)),
        ((nf, 2), (nf, 4)),
        (one, one),
        (one, (2,)),
        (one, (2,)),
        (one, one),
        (one, (2,)),
        (one, (2, 2)),
        (one, one),
    ):
        sems += [dma(send), dma(recv)]
    held = (
        pltpu.VMEM((2, d, rank), BF16),
        pltpu.VMEM((d, hl), BF16),
        pltpu.VMEM((nf, hl, dl), BF16),
        pltpu.VMEM((2, rank, hl), BF16),
        pltpu.VMEM((2, rl, hl), BF16),
        pltpu.VMEM((8, 128), F32),
        pltpu.VMEM((dl, hl), F32),
        pltpu.VMEM((hl, dl), F32),
        pltpu.VMEM((4, rl, hl), F32),
    )
    state = pl.pallas_call(
        functools.partial(exchange_kernel, nf, nr, scale),
        out_shape=held,
        in_specs=[hbm] * 12,
        out_specs=(vmem,) * len(held),
        scratch_shapes=[
            pltpu.VMEM((2, tokens, d), BF16),
            pltpu.VMEM((2, tokens, hl), BF16),
            pltpu.VMEM((hl, tokens), BF16),
            pltpu.VMEM((2, hl, d), BF16),
            pltpu.VMEM((2, nr, rank, pc), BF16),
            pltpu.VMEM((2, nr, rank, pc), BF16),
            pltpu.VMEM((2, rank, pc), BF16),
            pltpu.VMEM((2, nf, rl, pc), BF16),
            pltpu.VMEM((2 * nr, 8, pc), F32),
            dma((12,)),
        ] + sems,
        compiler_params=pltpu.CompilerParams(
            collective_id=0, has_side_effects=True, vmem_limit_bytes=VMEM_LIMIT
        ),
    )(
        *(
            pltpu.with_memory_space_constraint(a, pltpu.HBM)
            for a in (
                input_act, query_cot, out_cot, attn_out, query_w, out_w, query_factor, out_factor,
                first_q, second_q, first_o, second_o,
            )
        )
    )
    group = min(nf, max(1, 128 // dl))
    results = (query_w, out_w, query_w, out_w, first_q, second_q, first_o, second_o)
    return pl.pallas_call(
        functools.partial(apply_kernel, nf, nr, group, 2 * rank * hl * 2, scale),
        out_shape=tuple(sds(a.shape, F32) for a in results) + (sds((d, hl), BF16), sds((hl, d), BF16)),
        in_specs=[vmem] * len(held),
        out_specs=(hbm,) * 10,
        scratch_shapes=[
            pltpu.VMEM((hl, rank), BF16),
            pltpu.VMEM((2, dl, hl), F32),
            pltpu.VMEM((2, hl, dl), F32),
            pltpu.VMEM((4, rl, hl), F32),
            pltpu.VMEM((d, hl), BF16),
            pltpu.VMEM((hl, d), BF16),
            dma((10,)),
        ],
        compiler_params=pltpu.CompilerParams(vmem_limit_bytes=VMEM_LIMIT),
    )(*state)


def solution(mesh):
    return jax.shard_map(
        functools.partial(body, mesh.shape["fs"], mesh.shape["rep"]),
        mesh=mesh,
        in_specs=(
            P(("fs", "rep"), None),
            P(("fs", "rep"), "tp"),
            P(("fs", "rep"), None),
            P(("fs", "rep"), "tp"),
            P("fs", "tp"),
            P("tp", "fs"),
            P("fs", None),
            P("fs", None),
            P("fs", "tp"),
            P("fs", "tp"),
            P("fs", "tp"),
            P("fs", "tp"),
        ),
        out_specs=(
            P("fs", "tp"),
            P("tp", "fs"),
            P("fs", "tp"),
            P("tp", "fs"),
            P("fs", "tp"),
            P("fs", "tp"),
            P("fs", "tp"),
            P("fs", "tp"),
            P(None, "tp"),
            P("tp", None),
        ),
        check_vma=False,
    )
```

```python
import functools
import math

import jax
import jax.numpy as jnp
from jax import lax
from jax.experimental import pallas as pl
from jax.experimental.pallas import tpu as pltpu
from jax.sharding import PartitionSpec as P

MESH = pl.DeviceIdType.MESH
F32 = jnp.float32
BF16 = jnp.bfloat16
VMEM_LIMIT = 40 << 20
W_Q, W_O = (0, 2), (1, 3)


def rcopy(src, dst, sems, index, there, **where):
    return pltpu.make_async_remote_copy(
        src_ref=src,
        dst_ref=dst,
        send_sem=sems[0].at[index],
        recv_sem=sems[1].at[there],
        device_id=where,
        device_id_type=MESH,
    )


def nt_dot(a, b):
    return lax.dot_general(a, b, (((1,), (1,)), ((), ())), preferred_element_type=F32)


def exchange_kernel(
    nf, nr, scale,
    x_ref, cq_ref, y_ref, ca_ref, wq_ref, wo_ref, fq_ref, fo_ref, m1q_ref, m2q_ref, m1o_ref, m2o_ref,
    fall, wq_out, wo_out, dir_all, sq_out, w32q, w32o, moms,
    acts, cots, cot_t, grads, pieces, piece_in, summed, summed_in, proj_own, sq_all,
    loc, fa_s, fa_r, fb_s, fb_r, fc_s, fc_r, wz_s, wz_r, wx_s, wx_r, ps_s, ps_r, ss_s, ss_r,
    da_s, da_r, db_s, db_r, sq_s, sq_r,
):
    f, r, t = lax.axis_index("fs"), lax.axis_index("rep"), lax.axis_index("tp")
    ot = 1 - t
    dl, rank = fq_ref.shape
    hl = cq_ref.shape[1]
    dq, ch, pc, rl = dl // nr, rank // 2, hl // nr, rank // nf
    dh, hh = dl // 2, hl // 2
    fa, fb, fc = (fa_s, fa_r), (fb_s, fb_r), (fc_s, fc_r)
    wz, wx = (wz_s, wz_r), (wx_s, wx_r)
    ps, ss, da, db, sq = (ps_s, ps_r), (ss_s, ss_r), (da_s, da_r), (db_s, db_r), (sq_s, sq_r)

    def fpeer(k):
        return lax.rem(f + k, nf)

    def rpeer(j):
        return lax.rem(r + j, nr)

    def each_f(body):
        lax.fori_loop(1, nf, lambda k, _: (body(fpeer(k)), 0)[1], 0)

    def rows(start, size):
        return pl.ds(pl.multiple_of(start, 16), size)

    def pcols(part):
        return pl.ds(pl.multiple_of(part * pc, pc), pc)

    def local(i, src, dst):
        return pltpu.make_async_copy(src, dst, loc.at[i])

    own_rows = rows(f * dl, dl)
    load_f = [local(0, fq_ref, fall.at[0, own_rows]), local(1, fo_ref, fall.at[1, own_rows])]
    load_w = [local(2, wq_ref, w32q), local(3, wo_ref, w32o)]
    load_c = [local(4, cq_ref, cots.at[0]), local(5, ca_ref, cots.at[1])]
    load_x = [local(6, x_ref, acts.at[0]), local(7, y_ref, acts.at[1])]
    load_m = [local(8 + n, ref, moms.at[n]) for n, ref in enumerate((m1q_ref, m2q_ref, m1o_ref, m2o_ref))]
    for c in load_f + load_w + [load_c[0], load_x[0], load_c[1], load_x[1]] + load_m:
        c.start()

    barrier = pltpu.get_barrier_semaphore()
    each_f(lambda p: pl.semaphore_signal(barrier, inc=1, device_id={"fs": p}, device_id_type=MESH))
    for j in range(1, nr):
        pl.semaphore_signal(barrier, inc=1, device_id={"rep": rpeer(j)}, device_id_type=MESH)
    for j in range(nr):
        pl.semaphore_signal(barrier, inc=1, device_id={"rep": rpeer(j), "tp": ot}, device_id_type=MESH)
    pl.semaphore_wait(barrier, nf - 1 + 2 * nr - 1)

    def line(k, act):
        for up in (0, 1):
            p = f - k if up else f + k

            @pl.when(p >= 0 if up else p < nf)
            def _():
                act(p, up)

    def each_line(act):
        lax.fori_loop(1, nf, lambda k, _: (line(k, act), 0)[1], 0)

    def onward(up):
        return f < nf - 1 if up else f > 0

    half = (lax.rem(r, 2), r // (nr // 2))
    mate = (r + 1 - 2 * half[0], lax.rem(r + nr // 2, nr))

    def hops(i):
        return ((r, mate[i], 0), (r, mate[1 - i], 1), (mate[i], mate[1 - i], 1))

    def fcols(core):
        return pl.ds(pl.multiple_of(core * ch, ch), ch)

    def fchunk(i, core, block, part, count=1):
        return fall.at[i, rows(block * dl + part * dq, count * dq), fcols(core)]

    def fa_copy(i, p, up):
        piece = fchunk(i, t, p, r)
        return rcopy(piece, piece, fa, (p, up), (i, p), fs=f + 1 if up else f - 1)

    def fb_copy(i, p, n):
        part, to, slot = hops(i)[n]
        return rcopy(fchunk(i, t, p, part), fchunk(i, t, p, part), fb, 0, (i, p, slot), rep=to)

    def fb_wait(i, p, slot):
        there = fchunk(i, t, p, 0, 1 + slot)
        rcopy(there, there, fb, 0, (i, p, slot), rep=mate[0]).wait_recv()

    def fc_copy(i, core, p):
        block = fall.at[i, rows(p * dl, dl), fcols(core)]
        return rcopy(block, block, fc, 0, (i, p), tp=ot)

    def arrive_f(i, p, up):
        fa_copy(i, p, up).wait_recv()
        pl.when(onward(up))(lambda: fa_copy(i, p, up).start())
        for n in range(2):
            fb_copy(i, p, n).start()

    def relay_f(i, p):
        fb_wait(i, p, 0)
        fb_copy(i, p, 2).start()

    def across_f(i, p):
        fb_wait(i, p, 1)
        fc_copy(i, t, p).start()

    def rest_f(i):
        each_line(lambda p, up: fc_copy(i, ot, p).wait_recv())

    def w_piece(p, j, h):
        size = (dh, hh)[j % 2]
        start = h * size + j // 2 * (size // 2)
        if j % 2 == 0:
            return wq_out.at[rows(p * dl + start, size // 2)]
        return wo_out.at[p, rows(start, size // 2)]

    def wz_copy(p, j, up):
        piece = w_piece(p, j, half[j % 2])
        return rcopy(piece, piece, wz, (p, up), (p, j), fs=f + 1 if up else f - 1)

    def wx_copy(p, j):
        piece = w_piece(p, j, half[j % 2])
        return rcopy(piece, piece, wx, 0, 0, rep=mate[j % 2])

    def w_step(k, parts, wait=True, ahead=True, plane=True):
        for j in parts:
            def act(p, up):
                if wait:
                    wz_copy(p, j, up).wait_recv()
                if ahead:
                    pl.when(onward(up))(lambda: wz_copy(p, j, up).start())
                if plane:
                    wx_copy(p, j).start()

            line(k, act)

    for c in load_f:
        c.wait()
    for i in range(2):
        for up in (0, 1):
            pl.when(onward(up))(lambda: fa_copy(i, f, up).start())

    for c in load_w:
        c.wait()
    wq_out[own_rows, :] = w32q[...].astype(BF16)
    wo_out[f] = w32o[...].astype(BF16)
    nb = min(512, x_ref.shape[1])

    def turn(i):
        load_c[i].wait()
        cot_t[...] = cots[i].T
        load_x[i].wait()

    def columns(i, first, last):
        def column(n, _):
            cols = pl.ds(pl.multiple_of(n * nb, nb), nb)
            grads[i, :, cols] = jnp.dot(cot_t[...], acts[i, :, cols], preferred_element_type=F32).astype(BF16)
            return 0

        lax.fori_loop(first, last, column, 0)

    nc = x_ref.shape[1] // nb

    def ps_copy(i, j, core):
        q = rpeer(j)
        return rcopy(pieces.at[i, q, fcols(core)], piece_in.at[i, r, fcols(core)], ps, 0, i, rep=q)

    def project(i, core):
        term = jnp.dot(grads[i], fall[i, :, fcols(core)], preferred_element_type=F32).T.astype(BF16)
        for part in range(nr):
            pieces[i, part, fcols(core), :] = term[:, part * pc:(part + 1) * pc]
        for j in range(1, nr):
            ps_copy(i, j, core).start()

    def ss_copy(i, p):
        return rcopy(summed.at[i, rows(p * rl, rl)], summed_in.at[i, f], ss, 0, i, fs=p)

    def reduce_rep(i):
        there = piece_in.at[i, pl.ds(0, nr - 1)]
        rcopy(there, there, ps, 0, i, rep=mate[0]).wait_recv()
        total = pieces[i, r].astype(F32)
        for j in range(1, nr):
            total = total + piece_in[i, rpeer(j)].astype(F32)
        summed[i] = total.astype(BF16)
        each_f(lambda p: ss_copy(i, p).start())

    own_rank = rows(f * rl, rl)

    def da_copy(i, p):
        own = dir_all.at[i, own_rank, pcols(r)]
        return rcopy(own, own, da, i, i, fs=p)

    def direction(i):
        there = summed_in.at[i, pl.ds(0, nf - 1)]
        rcopy(there, there, ss, 0, i, fs=fpeer(1)).wait_recv()

        def gather_sum(k, total):
            return total + summed_in[i, fpeer(k)].astype(F32)

        proj = lax.fori_loop(1, nf, gather_sum, summed[i, own_rank, :].astype(F32)).astype(BF16)
        proj_own[i] = proj
        proj = proj.astype(F32) * scale
        load_m[2 * i].wait()
        load_m[2 * i + 1].wait()
        first = 0.8 * moms[2 * i, :, pcols(r)] + 0.2 * proj
        second = 0.9 * moms[2 * i + 1, :, pcols(r)] + 0.1 * proj * proj
        dir_all[i, own_rank, pcols(r)] = (first / jnp.sqrt(second)).astype(BF16)
        each_f(lambda p: da_copy(i, p).start())

    def da_waits(i):
        there = dir_all.at[i, pl.ds(0, (nf - 1) * rl), pl.ds(0, pc)]
        rcopy(there, there, da, i, i, fs=fpeer(1)).wait()
        d = dir_all[i, :, pcols(r)].astype(F32)
        dir_all[i, own_rank, pcols(r)] = proj_own[i]
        return jnp.sum((d * d).reshape(rank // 8, 8, pc), axis=0)

    def db_copy(i, n):
        part, to, slot = hops(i)[n]
        piece = dir_all.at[i, :, pcols(part)]
        return rcopy(piece, piece, db, 0, (i, slot), rep=to)

    def db_wait(i, slot):
        there = dir_all.at[i, :, pl.ds(0, (1 + slot) * pc)]
        rcopy(there, there, db, 0, (i, slot), rep=mate[0]).wait_recv()

    def spread(i):
        for n in range(2):
            db_copy(i, n).start()

    def spread_on(i):
        db_wait(i, 0)
        db_copy(i, 2).start()

    peers = [(j, c) for j in range(nr) for c in range(2) if j + c > 0]

    def sq_copy(j, c):
        own = sq_all.at[2 * r + t]
        return rcopy(own, own, sq, 0, 0, rep=rpeer(j), tp=(t, ot)[c])

    def squares(total):
        sq_all[2 * r + t] = total
        for j, c in peers:
            sq_copy(j, c).start()

    inner = jnp.logical_and(f > 0, f < nf - 1)

    def w_own(k):
        for up in (0, 1):
            @pl.when(jnp.logical_and(onward(up), (f if up else nf - 1 - f) == k))
            def _():
                for j in W_Q + W_O:
                    wz_copy(f, j, up).start()

    def forward_f():
        def step(k, _):
            line(k, functools.partial(arrive_f, 0))
            line(k, functools.partial(arrive_f, 1))
            w_own(k)
            line(k - 1, lambda p, up: relay_f(0, p))
            return 0

        lax.fori_loop(2, nf, step, 0)
        line(nf - 1, lambda p, up: relay_f(0, p))

    def finish_f():
        def step(p, up):
            across_f(0, p)
            relay_f(1, p)

        each_line(step)

    w_own(0)
    turn(0)
    columns(0, 0, nc)
    line(1, functools.partial(arrive_f, 0))
    turn(1)
    columns(1, 0, nc // 4)
    line(1, functools.partial(arrive_f, 1))
    w_own(1)
    columns(1, nc // 4, nc)
    forward_f()
    finish_f()
    project(0, t)
    w_step(1, W_Q[:1], plane=False)
    rest_f(0)
    project(0, ot)
    w_step(1, W_Q[1:], plane=False)
    each_line(lambda p, up: across_f(1, p))
    project(1, t)
    rest_f(1)
    project(1, ot)
    w_step(1, W_O, ahead=False, plane=False)
    pl.when(t == 1)(lambda: w_step(1, W_O, wait=False, plane=False))
    w_step(1, W_Q + W_O, wait=False, ahead=False)
    reduce_rep(0)
    pl.when(t == 0)(lambda: w_step(1, W_O, wait=False, plane=False))
    reduce_rep(1)
    pl.when(~inner)(lambda: w_step(2, W_Q, ahead=False))
    direction(0)
    pl.when(~inner)(lambda: w_step(2, W_O, ahead=False))
    direction(1)
    pl.when(~inner)(lambda: w_step(2, W_Q + W_O, wait=False, plane=False))
    pl.when(inner)(lambda: w_step(2, W_Q + W_O, plane=False))
    total = da_waits(0)
    spread(0)
    squares(total + da_waits(1))
    spread(1)

    def w_steps(parts):
        lax.fori_loop(3, max(3, nf), lambda k, _: (w_step(k, parts), 0)[1], 0)

    pl.when(inner)(lambda: w_step(2, W_Q, wait=False, ahead=False))
    spread_on(0)
    pl.when(inner)(lambda: w_step(2, W_O, wait=False, ahead=False))
    w_steps(W_Q)
    spread_on(1)
    w_steps(W_O)

    def finish():
        for i in range(2):
            db_wait(i, 1)
        there = sq_all.at[pl.ds(0, 2 * nr - 1)]
        rcopy(there, there, sq, 0, 0, tp=ot).wait()
        total = sq_all[0]
        for n in range(1, 2 * nr):
            total = total + sq_all[n]
        sq_out[...] = jnp.zeros(sq_out.shape, F32) + jnp.sum(total)

    finish()

    def rest_w():
        there = wq_out.at[pl.ds(0, (nf - 1) * dl)]
        rcopy(there, there, wx, 0, 0, rep=mate[0]).wait()

    rest_w()

    def drain():
        def blocks(p, _):
            for up in (0, 1):
                def sent_on():
                    sent = wq_out.at[rows(p * dl, dl)]
                    rcopy(sent, sent, wz, (p, up), (p, 0), fs=fpeer(1)).wait_send()
                    sent = fall.at[:, pl.ds(0, dq), fcols(0)]
                    rcopy(sent, sent, fa, (p, up), (0, p), fs=fpeer(1)).wait_send()

                pl.when(jnp.logical_and(onward(up), p <= f if up else p >= f))(sent_on)
            return 0

        lax.fori_loop(0, nf, blocks, 0)
        for sent, sems in (
            (fall.at[:, pl.ds(0, 3 * (nf - 1) * dq), fcols(0)], fb),
            (fall.at[:, pl.ds(0, (nf - 1) * dl), fcols(0)], fc),
            (pieces.at[:, pl.ds(0, nr - 1)], ps),
            (summed.at[:, pl.ds(0, (nf - 1) * rl)], ss),
            (dir_all.at[:, :, pl.ds(0, 3 * pc)], db),
        ):
            rcopy(sent, sent, (sems[0], sems[0]), 0, 0, tp=ot).wait_send()

    drain()


def apply_kernel(
    nf, nr, group, count, scale,
    fall, wq, wo, dir_ref, sq_ref, w32q, w32o, moms,
    nwq_out, nwo_out, sq_out, so_out, n1q_out, n2q_out, n1o_out, n2o_out, cq_out, co_out,
    dirs, dir_t, stage_q, stage_o, stage_m, copy_q, copy_o, sems,
):
    f = lax.axis_index("fs")
    dl, hl = w32q.shape
    inverse = 1.0 / jnp.sqrt(sq_ref[0:1, 0:1] / count + 1e-06)

    def out(i, src, dst):
        copy = pltpu.make_async_copy(src, dst, sems.at[i])
        copy.start()
        return copy

    rl = moms.shape[1]
    own_rank = pl.ds(pl.multiple_of(f * rl, rl), rl)
    sent = []
    for i, (first_out, second_out) in enumerate(((n1q_out, n2q_out), (n1o_out, n2o_out))):
        scaled = dir_ref[i, own_rank, :].astype(F32) * scale
        first = 0.8 * moms[2 * i] + 0.2 * scaled
        second = 0.9 * moms[2 * i + 1] + 0.1 * scaled * scaled
        stage_m[2 * i], stage_m[2 * i + 1] = first, second
        dirs[i] = dir_ref[i]
        dirs[i, own_rank, :] = (first / jnp.sqrt(second)).astype(BF16)
        sent += [out(2 * i, stage_m.at[2 * i], first_out), out(2 * i + 1, stage_m.at[2 * i + 1], second_out)]

    own = pl.ds(pl.multiple_of(f * dl, dl), dl)
    step_q = jnp.dot(fall[0, own, :], dirs[0], preferred_element_type=F32) * inverse
    stage_q[0] = step_q
    sent += [out(4, stage_q.at[0], sq_out)]
    stage_q[1] = w32q[...] - 0.01 * step_q
    sent += [out(5, stage_q.at[1], nwq_out)]
    dir_t[...] = dirs[1].T
    step_o = nt_dot(dir_t[...], fall[1, own, :]) * inverse
    stage_o[0] = step_o
    sent += [out(6, stage_o.at[0], so_out)]
    stage_o[1] = w32o[...] - 0.01 * step_o
    sent += [out(7, stage_o.at[1], nwo_out)]

    size = group * dl

    def finish_q(part, step):
        copy_q[part, :] = (wq[part, :].astype(F32) - 0.01 * step).astype(BF16)
        pltpu.make_async_copy(copy_q.at[part], cq_out.at[part], sems.at[8]).start()

    def finish_o(g, part, step):
        weight = jnp.concatenate([wo[g * group + m] for m in range(group)], axis=1).astype(F32)
        copy_o[:, part] = (weight - 0.01 * step).astype(BF16)
        pltpu.make_async_copy(copy_o.at[:, part], co_out.at[:, part], sems.at[9]).start()

    def block(g):
        part = pl.ds(pl.multiple_of(g * size, size), size)
        finish_q(part, jnp.dot(fall[0, part, :], dirs[0], preferred_element_type=F32) * inverse)
        finish_o(g, part, nt_dot(dir_t[...], fall[1, part, :]) * inverse)

    if group == 1:
        finish_q(own, stage_q[0])
        finish_o(f, own, stage_o[0])
        lax.fori_loop(1, nf, lambda k, _: (block(lax.rem(f + k, nf)), 0)[1], 0)
    else:
        lax.fori_loop(0, nf // group, lambda g, _: (block(g), 0)[1], 0)
    pltpu.make_async_copy(copy_q, cq_out, sems.at[8]).wait()
    pltpu.make_async_copy(copy_o, co_out, sems.at[9]).wait()
    for copy in sent:
        copy.wait()


def body(
    nf, nr,
    input_act, query_cot, out_cot, attn_out, query_w, out_w, query_factor, out_factor,
    first_q, second_q, first_o, second_o,
):
    tokens, d = input_act.shape
    hl = query_cot.shape[1]
    dl, rank = query_factor.shape
    rl = first_q.shape[0]
    pc = hl // nr
    scale = 1.0 / math.sqrt(tokens * nf * nr)
    hbm = pl.BlockSpec(memory_space=pltpu.HBM)
    vmem = pl.BlockSpec(memory_space=pltpu.VMEM)
    dma = pltpu.SemaphoreType.DMA
    sds = jax.ShapeDtypeStruct
    one = (1,)
    sems = []
    for send, recv in (
        ((nf, 2), (2, nf)),
        (one, (2, nf, 2)),
        (one, (2, nf)),
        ((nf, 2), (nf, 4)),
        (one, one),
        (one, (2,)),
        (one, (2,)),
        ((2,), (2,)),
        (one, (2, 2)),
        (one, one),
    ):
        sems += [dma(send), dma(recv)]
    held = (
        pltpu.VMEM((2, d, rank), BF16),
        pltpu.VMEM((d, hl), BF16),
        pltpu.VMEM((nf, hl, dl), BF16),
        pltpu.VMEM((2, rank, hl), BF16),
        pltpu.VMEM((8, 128), F32),
        pltpu.VMEM((dl, hl), F32),
        pltpu.VMEM((hl, dl), F32),
        pltpu.VMEM((4, rl, hl), F32),
    )
    state = pl.pallas_call(
        functools.partial(exchange_kernel, nf, nr, scale),
        out_shape=held,
        in_specs=[hbm] * 12,
        out_specs=(vmem,) * len(held),
        scratch_shapes=[
            pltpu.VMEM((2, tokens, d), BF16),
            pltpu.VMEM((2, tokens, hl), BF16),
            pltpu.VMEM((hl, tokens), BF16),
            pltpu.VMEM((2, hl, d), BF16),
            pltpu.VMEM((2, nr, rank, pc), BF16),
            pltpu.VMEM((2, nr, rank, pc), BF16),
            pltpu.VMEM((2, rank, pc), BF16),
            pltpu.VMEM((2, nf, rl, pc), BF16),
            pltpu.VMEM((2, rl, pc), BF16),
            pltpu.VMEM((2 * nr, 8, pc), F32),
            dma((12,)),
        ] + sems,
        compiler_params=pltpu.CompilerParams(
            collective_id=0, has_side_effects=True, vmem_limit_bytes=VMEM_LIMIT
        ),
    )(
        *(
            pltpu.with_memory_space_constraint(a, pltpu.HBM)
            for a in (
                input_act, query_cot, out_cot, attn_out, query_w, out_w, query_factor, out_factor,
                first_q, second_q, first_o, second_o,
            )
        )
    )
    group = min(nf, max(1, 128 // dl))
    results = (query_w, out_w, query_w, out_w, first_q, second_q, first_o, second_o)
    return pl.pallas_call(
        functools.partial(apply_kernel, nf, nr, group, 2 * rank * hl * 2, scale),
        out_shape=tuple(sds(a.shape, F32) for a in results) + (sds((d, hl), BF16), sds((hl, d), BF16)),
        in_specs=[vmem] * len(held),
        out_specs=(hbm,) * 10,
        scratch_shapes=[
            pltpu.VMEM((2, rank, hl), BF16),
            pltpu.VMEM((hl, rank), BF16),
            pltpu.VMEM((2, dl, hl), F32),
            pltpu.VMEM((2, hl, dl), F32),
            pltpu.VMEM((4, rl, hl), F32),
            pltpu.VMEM((d, hl), BF16),
            pltpu.VMEM((hl, d), BF16),
            dma((10,)),
        ],
        compiler_params=pltpu.CompilerParams(vmem_limit_bytes=VMEM_LIMIT),
    )(*state)


def solution(mesh):
    return jax.shard_map(
        functools.partial(body, mesh.shape["fs"], mesh.shape["rep"]),
        mesh=mesh,
        in_specs=(
            P(("fs", "rep"), None),
            P(("fs", "rep"), "tp"),
            P(("fs", "rep"), None),
            P(("fs", "rep"), "tp"),
            P("fs", "tp"),
            P("tp", "fs"),
            P("fs", None),
            P("fs", None),
            P("fs", "tp"),
            P("fs", "tp"),
            P("fs", "tp"),
            P("fs", "tp"),
        ),
        out_specs=(
            P("fs", "tp"),
            P("tp", "fs"),
            P("fs", "tp"),
            P("tp", "fs"),
            P("fs", "tp"),
            P("fs", "tp"),
            P("fs", "tp"),
            P("fs", "tp"),
            P(None, "tp"),
            P("tp", None),
        ),
        check_vma=False,
    )
```

```python
import functools
import math

import jax
import jax.numpy as jnp
from jax import lax
from jax.experimental import pallas as pl
from jax.experimental.pallas import tpu as pltpu
from jax.sharding import PartitionSpec as P

MESH = pl.DeviceIdType.MESH
F32 = jnp.float32
BF16 = jnp.bfloat16
VMEM_LIMIT = 40 << 20
W_Q, W_O = (0, 2), (1, 3)
SUBS = 2


def rcopy(src, dst, sems, index, there, **where):
    return pltpu.make_async_remote_copy(
        src_ref=src,
        dst_ref=dst,
        send_sem=sems[0].at[index],
        recv_sem=sems[1].at[there],
        device_id=where,
        device_id_type=MESH,
    )


def nt_dot(a, b):
    return lax.dot_general(a, b, (((1,), (1,)), ((), ())), preferred_element_type=F32)


def exchange_kernel(
    nf, nr, scale,
    x_ref, cq_ref, y_ref, ca_ref, wq_ref, wo_ref, fq_ref, fo_ref, m1q_ref, m2q_ref, m1o_ref, m2o_ref,
    fall, wq_out, wo_out, dir_all, sq_out, w32q, w32o, moms,
    acts, cots, cot_t, grads, pieces, piece_in, summed, summed_in, proj_own, sq_all,
    loc, fa_s, fa_r, fb_s, fb_r, fc_s, fc_r, wz_s, wz_r, wx_s, wx_r, ps_s, ps_r, ss_s, ss_r,
    da_s, da_r, db_s, db_r, sq_s, sq_r,
):
    f, r, t = lax.axis_index("fs"), lax.axis_index("rep"), lax.axis_index("tp")
    ot = 1 - t
    dl, rank = fq_ref.shape
    hl = cq_ref.shape[1]
    dq, ch, pc, rl = dl // nr, rank // 2, hl // nr, rank // nf
    dh, hh = dl // 2, hl // 2
    ns = SUBS if ch % (128 * SUBS) == 0 else 1
    cs = ch // ns
    fa, fb, fc = (fa_s, fa_r), (fb_s, fb_r), (fc_s, fc_r)
    wz, wx = (wz_s, wz_r), (wx_s, wx_r)
    ps, ss, da, db, sq = (ps_s, ps_r), (ss_s, ss_r), (da_s, da_r), (db_s, db_r), (sq_s, sq_r)

    def fpeer(k):
        return lax.rem(f + k, nf)

    def rpeer(j):
        return lax.rem(r + j, nr)

    def each_f(body):
        lax.fori_loop(1, nf, lambda k, _: (body(fpeer(k)), 0)[1], 0)

    def rows(start, size):
        return pl.ds(pl.multiple_of(start, 16), size)

    def pcols(part):
        return pl.ds(pl.multiple_of(part * pc, pc), pc)

    def local(i, src, dst):
        return pltpu.make_async_copy(src, dst, loc.at[i])

    own_rows = rows(f * dl, dl)
    load_f = [local(0, fq_ref, fall.at[0, own_rows]), local(1, fo_ref, fall.at[1, own_rows])]
    load_w = [local(2, wq_ref, w32q), local(3, wo_ref, w32o)]
    load_c = [local(4, cq_ref, cots.at[0]), local(5, ca_ref, cots.at[1])]
    load_x = [local(6, x_ref, acts.at[0]), local(7, y_ref, acts.at[1])]
    load_m = [local(8 + n, ref, moms.at[n]) for n, ref in enumerate((m1q_ref, m2q_ref, m1o_ref, m2o_ref))]
    for c in load_f + load_w + [load_c[0], load_x[0], load_c[1], load_x[1]] + load_m:
        c.start()

    barrier = pltpu.get_barrier_semaphore()
    each_f(lambda p: pl.semaphore_signal(barrier, inc=1, device_id={"fs": p}, device_id_type=MESH))
    for j in range(1, nr):
        pl.semaphore_signal(barrier, inc=1, device_id={"rep": rpeer(j)}, device_id_type=MESH)
    for j in range(nr):
        pl.semaphore_signal(barrier, inc=1, device_id={"rep": rpeer(j), "tp": ot}, device_id_type=MESH)
    pl.semaphore_wait(barrier, nf - 1 + 2 * nr - 1)

    def line(k, act):
        for up in (0, 1):
            p = f - k if up else f + k

            @pl.when(p >= 0 if up else p < nf)
            def _():
                act(p, up)

    def each_line(act):
        lax.fori_loop(1, nf, lambda k, _: (line(k, act), 0)[1], 0)

    def onward(up):
        return f < nf - 1 if up else f > 0

    half = (lax.rem(r, 2), r // (nr // 2))
    mate = (r + 1 - 2 * half[0], lax.rem(r + nr // 2, nr))

    def hops(i):
        return ((r, mate[i], 0), (r, mate[1 - i], 1), (mate[i], mate[1 - i], 1))

    def fcols(core):
        return pl.ds(pl.multiple_of(core * ch, ch), ch)

    def fchunk(i, p, part, s):
        cols = pl.ds(pl.multiple_of(t * ch + s * cs, cs), cs)
        return fall.at[i, rows(p * dl + part * dq, dq), cols]

    def fa_copy(i, p, s, up):
        piece = fchunk(i, p, r, s)
        return rcopy(piece, piece, fa, (p, up), (i, p, s), fs=f + 1 if up else f - 1)

    def fb_copy(i, p, s, n):
        part, to, slot = hops(i)[n]
        piece = fchunk(i, p, part, s)
        return rcopy(piece, piece, fb, 0, (i, p, ns if slot else s), rep=to)

    def fc_copy(i, core, p):
        block = fall.at[i, rows(p * dl, dl), fcols(core)]
        return rcopy(block, block, fc, 0, (i, p), tp=ot)

    def arrive_f(i, p, up):
        for s in range(ns):
            fa_copy(i, p, s, up).wait_recv()
            pl.when(onward(up))(lambda: fa_copy(i, p, s, up).start())
            for n in range(2):
                fb_copy(i, p, s, n).start()

    def relay_f(i, p):
        for s in range(ns):
            there = fchunk(i, p, mate[i], s)
            rcopy(there, there, fb, 0, (i, p, s), rep=mate[0]).wait_recv()
            fb_copy(i, p, s, 2).start()

    def across_f(i, p):
        there = fall.at[i, rows(p * dl, 2 * dq), fcols(t)]
        rcopy(there, there, fb, 0, (i, p, ns), rep=mate[0]).wait_recv()
        fc_copy(i, t, p).start()

    def rest_f(i):
        each_line(lambda p, up: fc_copy(i, ot, p).wait_recv())

    def w_piece(p, j, h):
        size = (dh, hh)[j % 2]
        start = h * size + j // 2 * (size // 2)
        if j % 2 == 0:
            return wq_out.at[rows(p * dl + start, size // 2)]
        return wo_out.at[p, rows(start, size // 2)]

    def wz_copy(p, j, up):
        piece = w_piece(p, j, half[j % 2])
        return rcopy(piece, piece, wz, (p, up), (p, j), fs=f + 1 if up else f - 1)

    def wx_copy(p, j):
        piece = w_piece(p, j, half[j % 2])
        return rcopy(piece, piece, wx, 0, 0, rep=mate[j % 2])

    def w_step(k, parts, wait=True, ahead=True, plane=True):
        for j in parts:
            def act(p, up):
                if wait:
                    wz_copy(p, j, up).wait_recv()
                if ahead:
                    pl.when(onward(up))(lambda: wz_copy(p, j, up).start())
                if plane:
                    wx_copy(p, j).start()

            line(k, act)

    for c in load_f:
        c.wait()
    for i in range(2):
        for s in range(ns):
            for up in (0, 1):
                pl.when(onward(up))(lambda: fa_copy(i, f, s, up).start())

    for c in load_w:
        c.wait()
    wq_out[own_rows, :] = w32q[...].astype(BF16)
    wo_out[f] = w32o[...].astype(BF16)
    nb = min(512, x_ref.shape[1])

    def turn(i):
        load_c[i].wait()
        cot_t[...] = cots[i].T
        load_x[i].wait()

    def columns(i, first, last):
        def column(n, _):
            cols = pl.ds(pl.multiple_of(n * nb, nb), nb)
            grads[i, :, cols] = jnp.dot(cot_t[...], acts[i, :, cols], preferred_element_type=F32).astype(BF16)
            return 0

        lax.fori_loop(first, last, column, 0)

    nc = x_ref.shape[1] // nb

    def ps_copy(i, j, core):
        q = rpeer(j)
        return rcopy(pieces.at[i, q, fcols(core)], piece_in.at[i, r, fcols(core)], ps, 0, i, rep=q)

    def project(i, core):
        term = jnp.dot(grads[i], fall[i, :, fcols(core)], preferred_element_type=F32).T.astype(BF16)
        for part in range(nr):
            pieces[i, part, fcols(core), :] = term[:, part * pc:(part + 1) * pc]
        for j in range(1, nr):
            ps_copy(i, j, core).start()

    def ss_copy(i, p):
        return rcopy(summed.at[i, rows(p * rl, rl)], summed_in.at[i, f], ss, 0, i, fs=p)

    def reduce_rep(i):
        there = piece_in.at[i, pl.ds(0, nr - 1)]
        rcopy(there, there, ps, 0, i, rep=mate[0]).wait_recv()
        total = pieces[i, r].astype(F32)
        for j in range(1, nr):
            total = total + piece_in[i, rpeer(j)].astype(F32)
        summed[i] = total.astype(BF16)
        each_f(lambda p: ss_copy(i, p).start())

    own_rank = rows(f * rl, rl)

    def da_copy(i, p):
        own = dir_all.at[i, own_rank, pcols(r)]
        return rcopy(own, own, da, i, i, fs=p)

    def direction(i):
        there = summed_in.at[i, pl.ds(0, nf - 1)]
        rcopy(there, there, ss, 0, i, fs=fpeer(1)).wait_recv()

        def gather_sum(k, total):
            return total + summed_in[i, fpeer(k)].astype(F32)

        proj = lax.fori_loop(1, nf, gather_sum, summed[i, own_rank, :].astype(F32)).astype(BF16)
        proj_own[i] = proj
        proj = proj.astype(F32) * scale
        load_m[2 * i].wait()
        load_m[2 * i + 1].wait()
        first = 0.8 * moms[2 * i, :, pcols(r)] + 0.2 * proj
        second = 0.9 * moms[2 * i + 1, :, pcols(r)] + 0.1 * proj * proj
        dir_all[i, own_rank, pcols(r)] = (first / jnp.sqrt(second)).astype(BF16)
        each_f(lambda p: da_copy(i, p).start())

    def da_waits(i):
        there = dir_all.at[i, pl.ds(0, (nf - 1) * rl), pl.ds(0, pc)]
        rcopy(there, there, da, i, i, fs=fpeer(1)).wait()
        d = dir_all[i, :, pcols(r)].astype(F32)
        dir_all[i, own_rank, pcols(r)] = proj_own[i]
        return jnp.sum((d * d).reshape(rank // 8, 8, pc), axis=0)

    def db_copy(i, n, h):
        part, to, slot = hops(i)[n]
        piece = dir_all.at[i, fcols(h), pcols(part)]
        return rcopy(piece, piece, db, 0, (i, 2 if slot else h), rep=to)

    def spread(i):
        for h in range(2):
            for n in range(2):
                db_copy(i, n, h).start()

    def spread_on(i):
        for h in range(2):
            there = dir_all.at[i, fcols(h), pcols(0)]
            rcopy(there, there, db, 0, (i, h), rep=mate[0]).wait_recv()
            db_copy(i, 2, h).start()

    peers = [(j, c) for j in range(nr) for c in range(2) if j + c > 0]

    def sq_copy(j, c):
        own = sq_all.at[2 * r + t]
        return rcopy(own, own, sq, 0, 0, rep=rpeer(j), tp=(t, ot)[c])

    def squares(total):
        sq_all[2 * r + t] = total
        for j, c in peers:
            sq_copy(j, c).start()

    inner = jnp.logical_and(f > 0, f < nf - 1)

    def w_own(k):
        for up in (0, 1):
            @pl.when(jnp.logical_and(onward(up), (f if up else nf - 1 - f) == k))
            def _():
                for j in W_Q + W_O:
                    wz_copy(f, j, up).start()

    def forward_f():
        def step(k, _):
            line(k, functools.partial(arrive_f, 0))
            line(k, functools.partial(arrive_f, 1))
            w_own(k)
            line(k - 1, lambda p, up: relay_f(0, p))
            return 0

        lax.fori_loop(2, min(3, nf), step, 0)
        columns(1, nc // 2, 3 * nc // 4)
        lax.fori_loop(3, max(3, nf), step, 0)
        line(nf - 1, lambda p, up: relay_f(0, p))

    def finish_f():
        def step(p, up):
            across_f(0, p)
            relay_f(1, p)

        each_line(step)

    w_own(0)
    turn(0)
    columns(0, 0, nc)
    line(1, functools.partial(arrive_f, 0))
    turn(1)
    columns(1, 0, nc // 4)
    line(1, functools.partial(arrive_f, 1))
    w_own(1)
    columns(1, nc // 4, nc // 2)
    forward_f()
    columns(1, 3 * nc // 4, nc)
    finish_f()
    project(0, t)
    w_step(1, W_Q[:1], plane=False)
    rest_f(0)
    project(0, ot)
    w_step(1, W_Q[1:], plane=False)
    each_line(lambda p, up: across_f(1, p))
    project(1, t)
    rest_f(1)
    project(1, ot)
    w_step(1, W_O, ahead=False, plane=False)
    pl.when(t == 1)(lambda: w_step(1, W_O, wait=False, plane=False))
    w_step(1, W_Q + W_O, wait=False, ahead=False)
    reduce_rep(0)
    pl.when(t == 0)(lambda: w_step(1, W_O, wait=False, plane=False))
    reduce_rep(1)
    pl.when(~inner)(lambda: w_step(2, W_Q, ahead=False))
    direction(0)
    pl.when(~inner)(lambda: w_step(2, W_O, ahead=False))
    direction(1)
    pl.when(inner)(lambda: w_step(2, W_Q + W_O, plane=False))
    total = da_waits(0)
    spread(0)
    squares(total + da_waits(1))
    spread(1)

    def w_steps(parts):
        lax.fori_loop(3, max(3, nf), lambda k, _: (w_step(k, parts), 0)[1], 0)

    pl.when(inner & (t == 0))(lambda: w_step(2, W_Q, wait=False, ahead=False))
    spread_on(0)
    pl.when(inner & (t == 0))(lambda: w_step(2, W_O, wait=False, ahead=False))
    pl.when(inner & (t == 1))(lambda: w_step(2, W_Q, wait=False, ahead=False))
    w_steps(W_Q)
    spread_on(1)
    pl.when(inner & (t == 1))(lambda: w_step(2, W_O, wait=False, ahead=False))
    w_steps(W_O)

    def finish():
        for i in range(2):
            there = dir_all.at[i, :, pl.ds(0, 2 * pc)]
            rcopy(there, there, db, 0, (i, 2), rep=mate[0]).wait_recv()
        there = sq_all.at[pl.ds(0, 2 * nr - 1)]
        rcopy(there, there, sq, 0, 0, tp=ot).wait()
        total = sq_all[0]
        for n in range(1, 2 * nr):
            total = total + sq_all[n]
        sq_out[...] = jnp.zeros(sq_out.shape, F32) + jnp.sum(total)

    finish()

    def rest_w():
        there = wq_out.at[pl.ds(0, (nf - 1) * dl)]
        rcopy(there, there, wx, 0, 0, rep=mate[0]).wait()

    rest_w()

    def drain():
        def blocks(p, _):
            for up in (0, 1):
                def sent_on():
                    sent = wq_out.at[rows(p * dl, dl)]
                    rcopy(sent, sent, wz, (p, up), (p, 0), fs=fpeer(1)).wait_send()
                    sent = fall.at[:, pl.ds(0, dq), fcols(0)]
                    rcopy(sent, sent, fa, (p, up), (0, p, 0), fs=fpeer(1)).wait_send()

                pl.when(jnp.logical_and(onward(up), p <= f if up else p >= f))(sent_on)
            return 0

        lax.fori_loop(0, nf, blocks, 0)
        for sent, sems in (
            (fall.at[:, pl.ds(0, 3 * (nf - 1) * dq), fcols(0)], fb),
            (fall.at[:, pl.ds(0, (nf - 1) * dl), fcols(0)], fc),
            (pieces.at[:, pl.ds(0, nr - 1)], ps),
            (summed.at[:, pl.ds(0, (nf - 1) * rl)], ss),
            (dir_all.at[:, :, pl.ds(0, 3 * pc)], db),
        ):
            rcopy(sent, sent, (sems[0], sems[0]), 0, 0, tp=ot).wait_send()

    drain()


def apply_kernel(
    nf, nr, group, count, scale,
    fall, wq, wo, dir_ref, sq_ref, w32q, w32o, moms,
    nwq_out, nwo_out, sq_out, so_out, n1q_out, n2q_out, n1o_out, n2o_out, cq_out, co_out,
    dirs, dir_t, stage_q, stage_o, stage_m, copy_q, copy_o, sems,
):
    f = lax.axis_index("fs")
    dl, hl = w32q.shape
    inverse = 1.0 / jnp.sqrt(sq_ref[0:1, 0:1] / count + 1e-06)

    def out(i, src, dst):
        copy = pltpu.make_async_copy(src, dst, sems.at[i])
        copy.start()
        return copy

    rl = moms.shape[1]
    own_rank = pl.ds(pl.multiple_of(f * rl, rl), rl)
    sent = []
    for i, (first_out, second_out) in enumerate(((n1q_out, n2q_out), (n1o_out, n2o_out))):
        scaled = dir_ref[i, own_rank, :].astype(F32) * scale
        first = 0.8 * moms[2 * i] + 0.2 * scaled
        second = 0.9 * moms[2 * i + 1] + 0.1 * scaled * scaled
        stage_m[2 * i], stage_m[2 * i + 1] = first, second
        dirs[i] = dir_ref[i]
        dirs[i, own_rank, :] = (first / jnp.sqrt(second)).astype(BF16)
        sent += [out(2 * i, stage_m.at[2 * i], first_out), out(2 * i + 1, stage_m.at[2 * i + 1], second_out)]

    own = pl.ds(pl.multiple_of(f * dl, dl), dl)
    step_q = jnp.dot(fall[0, own, :], dirs[0], preferred_element_type=F32) * inverse
    stage_q[0] = step_q
    sent += [out(4, stage_q.at[0], sq_out)]
    stage_q[1] = w32q[...] - 0.01 * step_q
    sent += [out(5, stage_q.at[1], nwq_out)]
    dir_t[...] = dirs[1].T
    step_o = nt_dot(dir_t[...], fall[1, own, :]) * inverse
    stage_o[0] = step_o
    sent += [out(6, stage_o.at[0], so_out)]
    stage_o[1] = w32o[...] - 0.01 * step_o
    sent += [out(7, stage_o.at[1], nwo_out)]

    size = group * dl

    def finish_q(part, step):
        copy_q[part, :] = (wq[part, :].astype(F32) - 0.01 * step).astype(BF16)
        pltpu.make_async_copy(copy_q.at[part], cq_out.at[part], sems.at[8]).start()

    def finish_o(g, part, step):
        weight = jnp.concatenate([wo[g * group + m] for m in range(group)], axis=1).astype(F32)
        copy_o[:, part] = (weight - 0.01 * step).astype(BF16)
        pltpu.make_async_copy(copy_o.at[:, part], co_out.at[:, part], sems.at[9]).start()

    def block(g):
        part = pl.ds(pl.multiple_of(g * size, size), size)
        finish_q(part, jnp.dot(fall[0, part, :], dirs[0], preferred_element_type=F32) * inverse)
        finish_o(g, part, nt_dot(dir_t[...], fall[1, part, :]) * inverse)

    if group == 1:
        finish_q(own, stage_q[0])
        finish_o(f, own, stage_o[0])
        lax.fori_loop(1, nf, lambda k, _: (block(lax.rem(f + k, nf)), 0)[1], 0)
    else:
        lax.fori_loop(0, nf // group, lambda g, _: (block(g), 0)[1], 0)
    pltpu.make_async_copy(copy_q, cq_out, sems.at[8]).wait()
    pltpu.make_async_copy(copy_o, co_out, sems.at[9]).wait()
    for copy in sent:
        copy.wait()


def body(
    nf, nr,
    input_act, query_cot, out_cot, attn_out, query_w, out_w, query_factor, out_factor,
    first_q, second_q, first_o, second_o,
):
    tokens, d = input_act.shape
    hl = query_cot.shape[1]
    dl, rank = query_factor.shape
    rl = first_q.shape[0]
    pc = hl // nr
    scale = 1.0 / math.sqrt(tokens * nf * nr)
    hbm = pl.BlockSpec(memory_space=pltpu.HBM)
    vmem = pl.BlockSpec(memory_space=pltpu.VMEM)
    dma = pltpu.SemaphoreType.DMA
    sds = jax.ShapeDtypeStruct
    one = (1,)
    sems = []
    for send, recv in (
        ((nf, 2), (2, nf, SUBS)),
        (one, (2, nf, SUBS + 1)),
        (one, (2, nf)),
        ((nf, 2), (nf, 4)),
        (one, one),
        (one, (2,)),
        (one, (2,)),
        ((2,), (2,)),
        (one, (2, 3)),
        (one, one),
    ):
        sems += [dma(send), dma(recv)]
    held = (
        pltpu.VMEM((2, d, rank), BF16),
        pltpu.VMEM((d, hl), BF16),
        pltpu.VMEM((nf, hl, dl), BF16),
        pltpu.VMEM((2, rank, hl), BF16),
        pltpu.VMEM((8, 128), F32),
        pltpu.VMEM((dl, hl), F32),
        pltpu.VMEM((hl, dl), F32),
        pltpu.VMEM((4, rl, hl), F32),
    )
    state = pl.pallas_call(
        functools.partial(exchange_kernel, nf, nr, scale),
        out_shape=held,
        in_specs=[hbm] * 12,
        out_specs=(vmem,) * len(held),
        scratch_shapes=[
            pltpu.VMEM((2, tokens, d), BF16),
            pltpu.VMEM((2, tokens, hl), BF16),
            pltpu.VMEM((hl, tokens), BF16),
            pltpu.VMEM((2, hl, d), BF16),
            pltpu.VMEM((2, nr, rank, pc), BF16),
            pltpu.VMEM((2, nr, rank, pc), BF16),
            pltpu.VMEM((2, rank, pc), BF16),
            pltpu.VMEM((2, nf, rl, pc), BF16),
            pltpu.VMEM((2, rl, pc), BF16),
            pltpu.VMEM((2 * nr, 8, pc), F32),
            dma((12,)),
        ] + sems,
        compiler_params=pltpu.CompilerParams(
            collective_id=0, has_side_effects=True, vmem_limit_bytes=VMEM_LIMIT
        ),
    )(
        *(
            pltpu.with_memory_space_constraint(a, pltpu.HBM)
            for a in (
                input_act, query_cot, out_cot, attn_out, query_w, out_w, query_factor, out_factor,
                first_q, second_q, first_o, second_o,
            )
        )
    )
    group = min(nf, max(1, 128 // dl))
    results = (query_w, out_w, query_w, out_w, first_q, second_q, first_o, second_o)
    return pl.pallas_call(
        functools.partial(apply_kernel, nf, nr, group, 2 * rank * hl * 2, scale),
        out_shape=tuple(sds(a.shape, F32) for a in results) + (sds((d, hl), BF16), sds((hl, d), BF16)),
        in_specs=[vmem] * len(held),
        out_specs=(hbm,) * 10,
        scratch_shapes=[
            pltpu.VMEM((2, rank, hl), BF16),
            pltpu.VMEM((hl, rank), BF16),
            pltpu.VMEM((2, dl, hl), F32),
            pltpu.VMEM((2, hl, dl), F32),
            pltpu.VMEM((4, rl, hl), F32),
            pltpu.VMEM((d, hl), BF16),
            pltpu.VMEM((hl, d), BF16),
            dma((10,)),
        ],
        compiler_params=pltpu.CompilerParams(vmem_limit_bytes=VMEM_LIMIT),
    )(*state)


def solution(mesh):
    return jax.shard_map(
        functools.partial(body, mesh.shape["fs"], mesh.shape["rep"]),
        mesh=mesh,
        in_specs=(
            P(("fs", "rep"), None),
            P(("fs", "rep"), "tp"),
            P(("fs", "rep"), None),
            P(("fs", "rep"), "tp"),
            P("fs", "tp"),
            P("tp", "fs"),
            P("fs", None),
            P("fs", None),
            P("fs", "tp"),
            P("fs", "tp"),
            P("fs", "tp"),
            P("fs", "tp"),
        ),
        out_specs=(
            P("fs", "tp"),
            P("tp", "fs"),
            P("fs", "tp"),
            P("tp", "fs"),
            P("fs", "tp"),
            P("fs", "tp"),
            P("fs", "tp"),
            P("fs", "tp"),
            P(None, "tp"),
            P("tp", None),
        ),
        check_vma=False,
    )
```

```python
import functools
import math

import jax
import jax.numpy as jnp
from jax import lax
from jax.experimental import pallas as pl
from jax.experimental.pallas import tpu as pltpu
from jax.sharding import PartitionSpec as P

MESH = pl.DeviceIdType.MESH
F32 = jnp.float32
BF16 = jnp.bfloat16
VMEM_LIMIT = 40 << 20
W_Q, W_O = (0, 2), (1, 3)
SUBS = 2


def rcopy(src, dst, sems, index, there, **where):
    return pltpu.make_async_remote_copy(
        src_ref=src,
        dst_ref=dst,
        send_sem=sems[0].at[index],
        recv_sem=sems[1].at[there],
        device_id=where,
        device_id_type=MESH,
    )


def nt_dot(a, b):
    return lax.dot_general(a, b, (((1,), (1,)), ((), ())), preferred_element_type=F32)


def exchange_kernel(
    nf, nr, scale,
    x_ref, cq_ref, y_ref, ca_ref, wq_ref, wo_ref, fq_ref, fo_ref, m1q_ref, m2q_ref, m1o_ref, m2o_ref,
    fall, wq_out, wo_out, dir_all, sq_out, w32q, w32o, moms,
    acts, cots, cot_t, grads, pieces, piece_in, summed, summed_in, proj_own, sq_all,
    loc, fa_s, fa_r, fb_s, fb_r, fc_s, fc_r, wz_s, wz_r, wx_s, wx_r, ps_s, ps_r, ss_s, ss_r,
    da_s, da_r, db_s, db_r, sq_s, sq_r,
):
    f, r, t = lax.axis_index("fs"), lax.axis_index("rep"), lax.axis_index("tp")
    ot = 1 - t
    dl, rank = fq_ref.shape
    hl = cq_ref.shape[1]
    dq, ch, pc, rl = dl // nr, rank // 2, hl // nr, rank // nf
    dh, hh = dl // 2, hl // 2
    ns = SUBS if ch % (128 * SUBS) == 0 else 1
    cs = ch // ns
    fa, fb, fc = (fa_s, fa_r), (fb_s, fb_r), (fc_s, fc_r)
    wz, wx = (wz_s, wz_r), (wx_s, wx_r)
    ps, ss, da, db, sq = (ps_s, ps_r), (ss_s, ss_r), (da_s, da_r), (db_s, db_r), (sq_s, sq_r)

    def fpeer(k):
        return lax.rem(f + k, nf)

    def rpeer(j):
        return lax.rem(r + j, nr)

    def each_f(body):
        lax.fori_loop(1, nf, lambda k, _: (body(fpeer(k)), 0)[1], 0)

    def rows(start, size):
        return pl.ds(pl.multiple_of(start, 16), size)

    def pcols(part):
        return pl.ds(pl.multiple_of(part * pc, pc), pc)

    def local(i, src, dst):
        return pltpu.make_async_copy(src, dst, loc.at[i])

    own_rows = rows(f * dl, dl)
    load_f = [local(0, fq_ref, fall.at[0, own_rows]), local(1, fo_ref, fall.at[1, own_rows])]
    load_w = [local(2, wq_ref, w32q), local(3, wo_ref, w32o)]
    load_c = [local(4, cq_ref, cots.at[0]), local(5, ca_ref, cots.at[1])]
    load_x = [local(6, x_ref, acts.at[0]), local(7, y_ref, acts.at[1])]
    load_m = [local(8 + n, ref, moms.at[n]) for n, ref in enumerate((m1q_ref, m2q_ref, m1o_ref, m2o_ref))]
    for c in load_f + load_w + [load_c[0], load_x[0], load_c[1], load_x[1]] + load_m:
        c.start()

    barrier = pltpu.get_barrier_semaphore()
    each_f(lambda p: pl.semaphore_signal(barrier, inc=1, device_id={"fs": p}, device_id_type=MESH))
    for j in range(1, nr):
        pl.semaphore_signal(barrier, inc=1, device_id={"rep": rpeer(j)}, device_id_type=MESH)
    for j in range(nr):
        pl.semaphore_signal(barrier, inc=1, device_id={"rep": rpeer(j), "tp": ot}, device_id_type=MESH)
    pl.semaphore_wait(barrier, nf - 1 + 2 * nr - 1)

    def line(k, act):
        for up in (0, 1):
            p = f - k if up else f + k

            @pl.when(p >= 0 if up else p < nf)
            def _():
                act(p, up)

    def each_line(act):
        lax.fori_loop(1, nf, lambda k, _: (line(k, act), 0)[1], 0)

    def onward(up):
        return f < nf - 1 if up else f > 0

    half = (lax.rem(r, 2), r // (nr // 2))
    mate = (r + 1 - 2 * half[0], lax.rem(r + nr // 2, nr))

    def hops(i):
        return ((r, mate[i], 0), (r, mate[1 - i], 1), (mate[i], mate[1 - i], 1))

    def fcols(core):
        return pl.ds(pl.multiple_of(core * ch, ch), ch)

    def fchunk(i, p, part, s):
        cols = pl.ds(pl.multiple_of(t * ch + s * cs, cs), cs)
        return fall.at[i, rows(p * dl + part * dq, dq), cols]

    def fa_copy(i, p, s, up):
        piece = fchunk(i, p, r, s)
        return rcopy(piece, piece, fa, (p, up), (i, p, s), fs=f + 1 if up else f - 1)

    def fb_copy(i, p, s, n):
        part, to, slot = hops(i)[n]
        piece = fchunk(i, p, part, s)
        return rcopy(piece, piece, fb, 0, (i, p, ns if slot else s), rep=to)

    def fc_copy(i, core, p):
        block = fall.at[i, rows(p * dl, dl), fcols(core)]
        return rcopy(block, block, fc, 0, (i, p), tp=ot)

    def arrive_f(i, p, up):
        for s in range(ns):
            fa_copy(i, p, s, up).wait_recv()
            pl.when(onward(up))(lambda: fa_copy(i, p, s, up).start())
            for n in range(2):
                fb_copy(i, p, s, n).start()

    def relay_f(i, p):
        for s in range(ns):
            there = fchunk(i, p, mate[i], s)
            rcopy(there, there, fb, 0, (i, p, s), rep=mate[0]).wait_recv()
            fb_copy(i, p, s, 2).start()

    def across_f(i, p):
        there = fall.at[i, rows(p * dl, 2 * dq), fcols(t)]
        rcopy(there, there, fb, 0, (i, p, ns), rep=mate[0]).wait_recv()
        fc_copy(i, t, p).start()

    def rest_f(i):
        each_line(lambda p, up: fc_copy(i, ot, p).wait_recv())

    def w_piece(p, j, h):
        size = (dh, hh)[j % 2]
        start = h * size + j // 2 * (size // 2)
        if j % 2 == 0:
            return wq_out.at[rows(p * dl + start, size // 2)]
        return wo_out.at[p, rows(start, size // 2)]

    def wz_copy(p, j, up):
        piece = w_piece(p, j, half[j % 2])
        return rcopy(piece, piece, wz, (p, up), (p, j), fs=f + 1 if up else f - 1)

    def wx_copy(p, j):
        piece = w_piece(p, j, half[j % 2])
        return rcopy(piece, piece, wx, 0, 0, rep=mate[j % 2])

    def w_step(k, parts, wait=True, ahead=True, plane=True):
        for j in parts:
            def act(p, up):
                if wait:
                    wz_copy(p, j, up).wait_recv()
                if ahead:
                    pl.when(onward(up))(lambda: wz_copy(p, j, up).start())
                if plane:
                    wx_copy(p, j).start()

            line(k, act)

    for c in load_f:
        c.wait()
    for i in range(2):
        for s in range(ns):
            for up in (0, 1):
                pl.when(onward(up))(lambda: fa_copy(i, f, s, up).start())

    for c in load_w:
        c.wait()
    wq_out[own_rows, :] = w32q[...].astype(BF16)
    wo_out[f] = w32o[...].astype(BF16)
    nb = min(512, x_ref.shape[1])

    def turn(i):
        load_c[i].wait()
        cot_t[...] = cots[i].T
        load_x[i].wait()

    def columns(i, first, last):
        def column(n, _):
            cols = pl.ds(pl.multiple_of(n * nb, nb), nb)
            grads[i, :, cols] = jnp.dot(cot_t[...], acts[i, :, cols], preferred_element_type=F32).astype(BF16)
            return 0

        lax.fori_loop(first, last, column, 0)

    nc = x_ref.shape[1] // nb

    def ps_copy(i, j, core):
        q = rpeer(j)
        return rcopy(pieces.at[i, q, fcols(core)], piece_in.at[i, r, fcols(core)], ps, 0, i, rep=q)

    def project(i, core):
        term = jnp.dot(grads[i], fall[i, :, fcols(core)], preferred_element_type=F32).T.astype(BF16)
        for part in range(nr):
            pieces[i, part, fcols(core), :] = term[:, part * pc:(part + 1) * pc]
        for j in range(1, nr):
            ps_copy(i, j, core).start()

    def ss_copy(i, p):
        return rcopy(summed.at[i, rows(p * rl, rl)], summed_in.at[i, f], ss, 0, i, fs=p)

    def reduce_rep(i):
        there = piece_in.at[i, pl.ds(0, nr - 1)]
        rcopy(there, there, ps, 0, i, rep=mate[0]).wait_recv()
        total = pieces[i, r].astype(F32)
        for j in range(1, nr):
            total = total + piece_in[i, rpeer(j)].astype(F32)
        summed[i] = total.astype(BF16)
        each_f(lambda p: ss_copy(i, p).start())

    own_rank = rows(f * rl, rl)

    def da_copy(i, p):
        own = dir_all.at[i, own_rank, pcols(r)]
        return rcopy(own, own, da, i, i, fs=p)

    def direction(i):
        there = summed_in.at[i, pl.ds(0, nf - 1)]
        rcopy(there, there, ss, 0, i, fs=fpeer(1)).wait_recv()

        def gather_sum(k, total):
            return total + summed_in[i, fpeer(k)].astype(F32)

        proj = lax.fori_loop(1, nf, gather_sum, summed[i, own_rank, :].astype(F32)).astype(BF16)
        proj_own[i] = proj
        proj = proj.astype(F32) * scale
        load_m[2 * i].wait()
        load_m[2 * i + 1].wait()
        first = 0.8 * moms[2 * i, :, pcols(r)] + 0.2 * proj
        second = 0.9 * moms[2 * i + 1, :, pcols(r)] + 0.1 * proj * proj
        dir_all[i, own_rank, pcols(r)] = (first / jnp.sqrt(second)).astype(BF16)
        each_f(lambda p: da_copy(i, p).start())

    def da_waits(i):
        there = dir_all.at[i, pl.ds(0, (nf - 1) * rl), pl.ds(0, pc)]
        rcopy(there, there, da, i, i, fs=fpeer(1)).wait()
        d = dir_all[i, :, pcols(r)].astype(F32)
        dir_all[i, own_rank, pcols(r)] = proj_own[i]
        return jnp.sum((d * d).reshape(rank // 8, 8, pc), axis=0)

    def db_copy(i, n, h):
        part, to, slot = hops(i)[n]
        piece = dir_all.at[i, fcols(h), pcols(part)]
        return rcopy(piece, piece, db, 0, (i, 2 if slot else h), rep=to)

    def spread(i):
        for h in range(2):
            for n in range(2):
                db_copy(i, n, h).start()

    def spread_on(i):
        for h in range(2):
            there = dir_all.at[i, fcols(h), pcols(0)]
            rcopy(there, there, db, 0, (i, h), rep=mate[0]).wait_recv()
            db_copy(i, 2, h).start()

    peers = [(j, c) for j in range(nr) for c in range(2) if j + c > 0]

    def sq_copy(j, c):
        own = sq_all.at[2 * r + t]
        return rcopy(own, own, sq, 0, 0, rep=rpeer(j), tp=(t, ot)[c])

    def squares(total):
        sq_all[2 * r + t] = total
        for j, c in peers:
            sq_copy(j, c).start()

    inner = jnp.logical_and(f > 0, f < nf - 1)

    def w_own(k):
        for up in (0, 1):
            @pl.when(jnp.logical_and(onward(up), (f if up else nf - 1 - f) == k))
            def _():
                for j in W_Q + W_O:
                    wz_copy(f, j, up).start()

    def forward_f():
        def step(k, _):
            line(k, functools.partial(arrive_f, 0))
            line(k, functools.partial(arrive_f, 1))
            w_own(k)
            line(k - 1, lambda p, up: relay_f(0, p))
            return 0

        lax.fori_loop(2, min(3, nf), step, 0)
        columns(1, nc // 2, 3 * nc // 4)
        lax.fori_loop(3, max(3, nf), step, 0)
        line(nf - 1, lambda p, up: relay_f(0, p))

    def finish_f():
        def step(p, up):
            across_f(0, p)
            relay_f(1, p)

        each_line(step)

    w_own(0)
    turn(0)
    columns(0, 0, nc)
    line(1, functools.partial(arrive_f, 0))
    turn(1)
    columns(1, 0, nc // 4)
    line(1, functools.partial(arrive_f, 1))
    w_own(1)
    columns(1, nc // 4, nc // 2)
    forward_f()
    columns(1, 3 * nc // 4, nc)
    finish_f()
    project(0, t)
    w_step(1, W_Q[:1], plane=False)
    rest_f(0)
    project(0, ot)
    w_step(1, W_Q[1:], plane=False)
    each_line(lambda p, up: across_f(1, p))
    project(1, t)
    rest_f(1)
    project(1, ot)
    w_step(1, W_O, ahead=False, plane=False)
    pl.when(t == 1)(lambda: w_step(1, W_O, wait=False, plane=False))
    w_step(1, W_Q + W_O, wait=False, ahead=False)
    reduce_rep(0)
    pl.when(t == 0)(lambda: w_step(1, W_O, wait=False, plane=False))
    reduce_rep(1)
    pl.when(~inner)(lambda: w_step(2, W_Q, ahead=False))
    direction(0)
    pl.when(~inner)(lambda: w_step(2, W_O, ahead=False))
    direction(1)
    pl.when(inner)(lambda: w_step(2, W_Q + W_O, plane=False))
    total = da_waits(0)
    spread(0)
    squares(total + da_waits(1))
    spread(1)

    def w_steps(parts):
        lax.fori_loop(3, max(3, nf), lambda k, _: (w_step(k, parts), 0)[1], 0)

    pl.when(inner & (t == 0))(lambda: w_step(2, W_Q, wait=False, ahead=False))
    spread_on(0)
    pl.when(inner & (t == 0))(lambda: w_step(2, W_O, wait=False, ahead=False))
    pl.when(inner & (t == 1))(lambda: w_step(2, W_Q, wait=False, ahead=False))
    w_steps(W_Q)
    spread_on(1)
    pl.when(inner & (t == 1))(lambda: w_step(2, W_O, wait=False, ahead=False))
    w_steps(W_O)

    def finish():
        for i in range(2):
            there = dir_all.at[i, :, pl.ds(0, 2 * pc)]
            rcopy(there, there, db, 0, (i, 2), rep=mate[0]).wait_recv()
        there = sq_all.at[pl.ds(0, 2 * nr - 1)]
        rcopy(there, there, sq, 0, 0, tp=ot).wait()
        total = sq_all[0]
        for n in range(1, 2 * nr):
            total = total + sq_all[n]
        sq_out[...] = jnp.zeros(sq_out.shape, F32) + jnp.sum(total)

    finish()

    def rest_w():
        there = wq_out.at[pl.ds(0, (nf - 1) * dl)]
        rcopy(there, there, wx, 0, 0, rep=mate[0]).wait()

    rest_w()

    def drain():
        def blocks(p, _):
            for up in (0, 1):
                def sent_on():
                    sent = wq_out.at[rows(p * dl, dl)]
                    rcopy(sent, sent, wz, (p, up), (p, 0), fs=fpeer(1)).wait_send()
                    sent = fall.at[:, pl.ds(0, dq), fcols(0)]
                    rcopy(sent, sent, fa, (p, up), (0, p, 0), fs=fpeer(1)).wait_send()

                pl.when(jnp.logical_and(onward(up), p <= f if up else p >= f))(sent_on)
            return 0

        lax.fori_loop(0, nf, blocks, 0)
        for sent, sems in (
            (fall.at[:, pl.ds(0, 3 * (nf - 1) * dq), fcols(0)], fb),
            (fall.at[:, pl.ds(0, (nf - 1) * dl), fcols(0)], fc),
            (pieces.at[:, pl.ds(0, nr - 1)], ps),
            (summed.at[:, pl.ds(0, (nf - 1) * rl)], ss),
            (dir_all.at[:, :, pl.ds(0, 3 * pc)], db),
        ):
            rcopy(sent, sent, (sems[0], sems[0]), 0, 0, tp=ot).wait_send()

    drain()


def apply_kernel(
    nf, nr, group, count, scale,
    fall, wq, wo, dir_ref, sq_ref, w32q, w32o, moms,
    nwq_out, nwo_out, sq_out, so_out, n1q_out, n2q_out, n1o_out, n2o_out, cq_out, co_out,
    dirs, dir_t, stage_q, stage_o, stage_m, copy_q, copy_o, sems,
):
    f = lax.axis_index("fs")
    dl, hl = w32q.shape
    inverse = 1.0 / jnp.sqrt(sq_ref[0:1, 0:1] / count + 1e-06)

    def out(i, src, dst):
        copy = pltpu.make_async_copy(src, dst, sems.at[i])
        copy.start()
        return copy

    rl = moms.shape[1]
    own_rank = pl.ds(pl.multiple_of(f * rl, rl), rl)
    sent = []
    for i, (first_out, second_out) in enumerate(((n1q_out, n2q_out), (n1o_out, n2o_out))):
        scaled = dir_ref[i, own_rank, :].astype(F32) * scale
        first = 0.8 * moms[2 * i] + 0.2 * scaled
        second = 0.9 * moms[2 * i + 1] + 0.1 * scaled * scaled
        stage_m[2 * i], stage_m[2 * i + 1] = first, second
        dirs[i] = dir_ref[i]
        dirs[i, own_rank, :] = (first / jnp.sqrt(second)).astype(BF16)
        sent += [out(2 * i, stage_m.at[2 * i], first_out), out(2 * i + 1, stage_m.at[2 * i + 1], second_out)]

    own = pl.ds(pl.multiple_of(f * dl, dl), dl)
    step_q = jnp.dot(fall[0, own, :], dirs[0], preferred_element_type=F32) * inverse
    stage_q[0] = step_q
    sent += [out(4, stage_q.at[0], sq_out)]
    stage_q[1] = w32q[...] - 0.01 * step_q
    sent += [out(5, stage_q.at[1], nwq_out)]
    dir_t[...] = dirs[1].T
    step_o = nt_dot(dir_t[...], fall[1, own, :]) * inverse
    stage_o[0] = step_o
    sent += [out(6, stage_o.at[0], so_out)]
    stage_o[1] = w32o[...] - 0.01 * step_o
    sent += [out(7, stage_o.at[1], nwo_out)]

    size = group * dl

    def finish_q(part, step):
        copy_q[part, :] = (wq[part, :].astype(F32) - 0.01 * step).astype(BF16)
        pltpu.make_async_copy(copy_q.at[part], cq_out.at[part], sems.at[8]).start()

    def finish_o(g, part, step):
        weight = jnp.concatenate([wo[g * group + m] for m in range(group)], axis=1).astype(F32)
        copy_o[:, part] = (weight - 0.01 * step).astype(BF16)
        pltpu.make_async_copy(copy_o.at[:, part], co_out.at[:, part], sems.at[9]).start()

    def block(g):
        part = pl.ds(pl.multiple_of(g * size, size), size)
        finish_q(part, jnp.dot(fall[0, part, :], dirs[0], preferred_element_type=F32) * inverse)
        finish_o(g, part, nt_dot(dir_t[...], fall[1, part, :]) * inverse)

    if group == 1:
        finish_q(own, stage_q[0])
        finish_o(f, own, stage_o[0])
        for k in range(1, nf):
            block(lax.rem(f + k, nf))
    else:
        lax.fori_loop(0, nf // group, lambda g, _: (block(g), 0)[1], 0)
    pltpu.make_async_copy(copy_q, cq_out, sems.at[8]).wait()
    pltpu.make_async_copy(copy_o, co_out, sems.at[9]).wait()
    for copy in sent:
        copy.wait()


def body(
    nf, nr,
    input_act, query_cot, out_cot, attn_out, query_w, out_w, query_factor, out_factor,
    first_q, second_q, first_o, second_o,
):
    tokens, d = input_act.shape
    hl = query_cot.shape[1]
    dl, rank = query_factor.shape
    rl = first_q.shape[0]
    pc = hl // nr
    scale = 1.0 / math.sqrt(tokens * nf * nr)
    hbm = pl.BlockSpec(memory_space=pltpu.HBM)
    vmem = pl.BlockSpec(memory_space=pltpu.VMEM)
    dma = pltpu.SemaphoreType.DMA
    sds = jax.ShapeDtypeStruct
    one = (1,)
    sems = []
    for send, recv in (
        ((nf, 2), (2, nf, SUBS)),
        (one, (2, nf, SUBS + 1)),
        (one, (2, nf)),
        ((nf, 2), (nf, 4)),
        (one, one),
        (one, (2,)),
        (one, (2,)),
        ((2,), (2,)),
        (one, (2, 3)),
        (one, one),
    ):
        sems += [dma(send), dma(recv)]
    held = (
        pltpu.VMEM((2, d, rank), BF16),
        pltpu.VMEM((d, hl), BF16),
        pltpu.VMEM((nf, hl, dl), BF16),
        pltpu.VMEM((2, rank, hl), BF16),
        pltpu.VMEM((8, 128), F32),
        pltpu.VMEM((dl, hl), F32),
        pltpu.VMEM((hl, dl), F32),
        pltpu.VMEM((4, rl, hl), F32),
    )
    state = pl.pallas_call(
        functools.partial(exchange_kernel, nf, nr, scale),
        out_shape=held,
        in_specs=[hbm] * 12,
        out_specs=(vmem,) * len(held),
        scratch_shapes=[
            pltpu.VMEM((2, tokens, d), BF16),
            pltpu.VMEM((2, tokens, hl), BF16),
            pltpu.VMEM((hl, tokens), BF16),
            pltpu.VMEM((2, hl, d), BF16),
            pltpu.VMEM((2, nr, rank, pc), BF16),
            pltpu.VMEM((2, nr, rank, pc), BF16),
            pltpu.VMEM((2, rank, pc), BF16),
            pltpu.VMEM((2, nf, rl, pc), BF16),
            pltpu.VMEM((2, rl, pc), BF16),
            pltpu.VMEM((2 * nr, 8, pc), F32),
            dma((12,)),
        ] + sems,
        compiler_params=pltpu.CompilerParams(
            collective_id=0, has_side_effects=True, vmem_limit_bytes=VMEM_LIMIT
        ),
    )(
        *(
            pltpu.with_memory_space_constraint(a, pltpu.HBM)
            for a in (
                input_act, query_cot, out_cot, attn_out, query_w, out_w, query_factor, out_factor,
                first_q, second_q, first_o, second_o,
            )
        )
    )
    group = min(nf, max(1, 128 // dl))
    results = (query_w, out_w, query_w, out_w, first_q, second_q, first_o, second_o)
    return pl.pallas_call(
        functools.partial(apply_kernel, nf, nr, group, 2 * rank * hl * 2, scale),
        out_shape=tuple(sds(a.shape, F32) for a in results) + (sds((d, hl), BF16), sds((hl, d), BF16)),
        in_specs=[vmem] * len(held),
        out_specs=(hbm,) * 10,
        scratch_shapes=[
            pltpu.VMEM((2, rank, hl), BF16),
            pltpu.VMEM((hl, rank), BF16),
            pltpu.VMEM((2, dl, hl), F32),
            pltpu.VMEM((2, hl, dl), F32),
            pltpu.VMEM((4, rl, hl), F32),
            pltpu.VMEM((d, hl), BF16),
            pltpu.VMEM((hl, d), BF16),
            dma((10,)),
        ],
        compiler_params=pltpu.CompilerParams(vmem_limit_bytes=VMEM_LIMIT),
    )(*state)


def solution(mesh):
    return jax.shard_map(
        functools.partial(body, mesh.shape["fs"], mesh.shape["rep"]),
        mesh=mesh,
        in_specs=(
            P(("fs", "rep"), None),
            P(("fs", "rep"), "tp"),
            P(("fs", "rep"), None),
            P(("fs", "rep"), "tp"),
            P("fs", "tp"),
            P("tp", "fs"),
            P("fs", None),
            P("fs", None),
            P("fs", "tp"),
            P("fs", "tp"),
            P("fs", "tp"),
            P("fs", "tp"),
        ),
        out_specs=(
            P("fs", "tp"),
            P("tp", "fs"),
            P("fs", "tp"),
            P("tp", "fs"),
            P("fs", "tp"),
            P("fs", "tp"),
            P("fs", "tp"),
            P("fs", "tp"),
            P(None, "tp"),
            P("tp", None),
        ),
        check_vma=False,
    )
```
